1024 devices in a mesh: dp: 4 (over x), kv: 128 (over z, y), tp: 2 (over core).
Axes of the slice: x: 4, y: 8, z: 16, core: 2. Of those that a mesh axis runs over, the one named last changes fastest.
Arguments:
- tokens: bfloat16 [32, 2048], P('dp', 'kv'), may hold values from -6 to 6
- lengths: int32 [32], P('dp'), may hold values from 1 to 32767, as said below
- query_weight: bfloat16 [2048, 2048], P('kv', 'tp'), may hold values from -0.125 to 0.125
- key_weight: bfloat16 [2048, 256], P('kv', 'tp'), may hold values from -0.125 to 0.125
- value_weight: bfloat16 [2048, 256], P('kv', 'tp'), may hold values from -0.125 to 0.125
- query_gain: float32 [64], replicated, may hold values from 0.1 to 1.9
- key_gain: float32 [64], replicated, may hold values from 0.1 to 1.9
- lambdas: float32 [16], P('tp'), may hold values from 0.3 to 0.8
- head_gain: float32 [128], replicated, may hold values from 0.1 to 1.9
- out_weight: bfloat16 [2048, 2048], P('tp', 'kv'), may hold values from -0.125 to 0.125
- cache_keys: bfloat16 [32, 32768, 2, 128], P('dp', 'kv', 'tp'), may hold values from -400 to 400
- cache_values: bfloat16 [32, 32768, 2, 128], P('dp', 'kv', 'tp'), may hold values from -6 to 6
Outputs:
- mixed: bfloat16 [32, 2048], P('dp', 'kv')
- new_keys: bfloat16 [32, 2, 128], P('dp', 'tp')
- new_values: bfloat16 [32, 2, 128], P('dp', 'tp')
The draws below stay inside these ranges and needn't reach their ends.
Inputs may be any that keep to these rules, and one draw needn't show every extreme that they name: `lengths`: of each index of dp's 8 sequences, the first has 32512 or more cached positions, the second fewer than 16, the others half of 32768 or more.
All inputs are finite; a program needn't handle non-finite values.
Results may differ from the reference program's by a relative error of at most 0.023.
Values may be sent and summed in bfloat16 or wider, within the bound.
A program may use at most 64 MiB of HBM per device.

```python
import math
import jax
import jax.numpy as jnp
from jax import lax

D = 2048
HEADS = 16
KV_HEADS = 2
HEAD = 64
VALUE = 128
SEQ_DEV = 8
POS_DEV = 256
BATCH = 32
CTX = 32768
N_TP = 2


def draw_lengths(key, part):
    slot_index = jnp.arange(BATCH, dtype=jnp.int32) % SEQ_DEV
    longest = jax.random.randint(jax.random.fold_in(key, 11), (BATCH,), CTX - POS_DEV, CTX)
    shortest = jax.random.randint(jax.random.fold_in(key, 12), (BATCH,), 1, 16)
    drawn = jax.random.randint(jax.random.fold_in(key, 13), (BATCH,), CTX // 2, CTX)
    chosen = jnp.where(slot_index == 0, longest, jnp.where(slot_index == 1, shortest, drawn))
    return chosen.astype(jnp.int32)


def draw_cache_keys(key, part):
    shape = (BATCH, CTX, KV_HEADS, VALUE)
    base = jnp.clip(jax.random.normal(jax.random.fold_in(key, 21), shape, jnp.float32) * 1.75, -10.5, 10.5)
    position_ids = jnp.arange(CTX, dtype=jnp.int32)[None, :]
    chosen_place = jax.random.randint(jax.random.fold_in(key, 24), (BATCH, 1), 0, CTX // 2)
    picked = (position_ids == 0) | (position_ids == chosen_place)
    factor = jnp.exp(jax.random.uniform(jax.random.fold_in(key, 23), (BATCH, CTX), jnp.float32, minval=jnp.log(10.0), maxval=jnp.log(35.0)))
    base = jnp.where(picked[:, :, None, None], base * factor[:, :, None, None], base)
    return base.astype(jnp.bfloat16)


def block_levels(key, extent, shards, least, largest):
    level, own = 1.0, jax.random.fold_in(key, 6)
    for dim, parts in shards:
        heights = jnp.exp(jax.random.uniform(jax.random.fold_in(own, dim), (parts,), jnp.float32, least / len(shards), largest / len(shards)))
        level = level * jnp.repeat(heights, extent[dim] // parts).reshape([-1 if axis == dim else 1 for axis in range(len(extent))])
    return level


def bell_draw(stream_key, shape, spread, reach, shards=(), kind=jnp.bfloat16):
    drawn = jax.random.normal(stream_key, shape, jnp.float32) * spread
    if len(shards) > 0:
        drawn = block_levels(stream_key, shape, shards, -0.22, 0.18) * drawn
    return jnp.clip(drawn, min=-reach, max=reach).astype(kind)


def setup_inputs(seed: int = 0) -> dict:
    key_list = jax.random.split(jax.random.key(seed), 13)
    tokens = bell_draw(key_list[0], (BATCH, D), 1.0, 6.0, ((0, 4), (1, 128)))
    lengths = draw_lengths(jax.random.fold_in(key_list[12], 71), 0)
    query_weight = bell_draw(key_list[2], (D, HEADS * VALUE), D ** -0.5, 0.125, ((0, 128), (1, 2)))
    key_weight = bell_draw(key_list[3], (D, KV_HEADS * VALUE), D ** -0.5, 0.125, ((0, 128), (1, 2)))
    value_weight = bell_draw(key_list[4], (D, KV_HEADS * VALUE), D ** -0.5, 0.125, ((0, 128), (1, 2)))
    query_gain = jnp.clip(1.0 + 0.18 * jax.random.normal(key_list[5], (HEAD,), jnp.float32), 0.1, 1.9)
    key_gain = jnp.clip(1.0 + 0.18 * jax.random.normal(key_list[6], (HEAD,), jnp.float32), 0.1, 1.9)
    lambdas = jnp.clip(0.3 + 0.5 * jax.random.uniform(key_list[7], (HEADS,), jnp.float32) ** block_levels(key_list[7], (HEADS,), ((0, 2),), -0.2, 0.2), 0.3, 0.8)
    head_gain = jnp.clip(1.0 + 0.18 * jax.random.normal(key_list[8], (VALUE,), jnp.float32), 0.1, 1.9)
    out_weight = bell_draw(key_list[9], (HEADS * VALUE, D), (HEADS * VALUE) ** -0.5, 0.125, ((0, 2), (1, 128)))
    cache_keys = draw_cache_keys(jax.random.fold_in(key_list[12], 71), 0)
    cache_values = bell_draw(key_list[11], (BATCH, CTX, KV_HEADS, VALUE), 1.0, 6.0, ((0, 4), (1, 128), (2, 2)))
    return {"tokens": tokens, "lengths": lengths, "query_weight": query_weight, "key_weight": key_weight, "value_weight": value_weight, "query_gain": query_gain, "key_gain": key_gain, "lambdas": lambdas, "head_gain": head_gain, "out_weight": out_weight, "cache_keys": cache_keys, "cache_values": cache_values}


epsilon = 1e-06
rotary_base = 10000.0
masked_score = -1e+30
output_scale = 0.2 + 0.6 * math.exp(-0.3)

def new_entries(proj_query, proj_key, proj_value, query_gain, key_gain, lengths):
    rows = proj_query.shape[0]
    head_dim = query_gain.shape[0]
    half_dim = head_dim // 2
    frequency = rotary_base ** (-jnp.arange(half_dim, dtype=jnp.float32) / half_dim)
    angle = lengths.astype(jnp.float32)[:, None, None, None] * frequency
    cosine_term = jnp.cos(angle)
    sine_term = jnp.sin(angle)

    def turned(pieces, gain):
        normed = pieces * lax.rsqrt(lax.optimization_barrier(jnp.mean(pieces * pieces, axis=-1, keepdims=True)) + epsilon) * gain
        lower_part = normed[..., :half_dim]
        upper_part = normed[..., half_dim:]
        return jnp.concatenate([lower_part * cosine_term - upper_part * sine_term, upper_part * cosine_term + lower_part * sine_term], axis=-1)
    queries = turned(proj_query.reshape(rows, -1, 2, head_dim), query_gain).astype(jnp.bfloat16)
    new_keys = turned(proj_key.reshape(rows, -1, 2, head_dim), key_gain).astype(jnp.bfloat16)
    new_values = proj_value.reshape(rows, -1, 2 * head_dim).astype(jnp.bfloat16)
    return (queries, new_keys.reshape(rows, -1, 2 * head_dim), new_values)

def finish_heads(weighted, totals, lambdas, head_gain):
    heads = weighted / totals[..., None]
    gaps = heads[..., 0, :] - lambdas[..., None] * heads[..., 1, :]
    normed = gaps * lax.rsqrt(lax.optimization_barrier(jnp.mean(gaps * gaps, axis=-1, keepdims=True)) + epsilon) * head_gain
    return (normed * output_scale).astype(jnp.bfloat16)

def attend_one(query, keys, values, length, own_key, own_value, lambdas, head_gain):
    positions, kv_heads, width = keys.shape
    head_dim = width // 2
    scale = head_dim ** (-0.5)
    query_wide = query.astype(jnp.float32)
    scores = jnp.einsum('kgtd,pktd->kgtp', query_wide, keys.reshape(positions, kv_heads, 2, head_dim).astype(jnp.float32)) * scale
    valid = jnp.arange(positions, dtype=jnp.int32) < length
    own_score = jnp.einsum('kgtd,ktd->kgt', query_wide, own_key.reshape(kv_heads, 2, head_dim).astype(jnp.float32)) * scale
    highest = jnp.maximum(lax.optimization_barrier(jnp.max(jnp.where(valid, scores, masked_score), axis=-1)), own_score)
    expo = jnp.where(valid, jnp.exp(scores - highest[..., None]), 0.0)
    own_weight = jnp.exp(own_score - highest)
    totals = lax.optimization_barrier(jnp.sum(expo, axis=-1)) + own_weight
    rounded = lax.optimization_barrier(expo.astype(jnp.bfloat16)).astype(jnp.float32)
    weighted = jnp.einsum('kgtp,pke->kgte', rounded, values.astype(jnp.float32))
    weighted = weighted + own_weight[..., None] * own_value.astype(jnp.float32)[:, None, None, :]
    attended = finish_heads(weighted, totals, lambdas.reshape(kv_heads, -1), head_gain)
    return attended.reshape(-1)

def reference(tokens, lengths, query_weight, key_weight, value_weight, query_gain, key_gain, lambdas, head_gain, out_weight, cache_keys, cache_values):
    proj_query = jnp.dot(tokens, query_weight, preferred_element_type=jnp.float32)
    proj_key = jnp.dot(tokens, key_weight, preferred_element_type=jnp.float32)
    proj_value = jnp.dot(tokens, value_weight, preferred_element_type=jnp.float32)
    queries, new_keys, new_values = new_entries(proj_query, proj_key, proj_value, query_gain, key_gain, lengths)
    rows = tokens.shape[0]
    kv_heads = cache_keys.shape[2]
    queries = queries.reshape(rows, kv_heads, -1, 2, queries.shape[-1])
    attended = lax.map(lambda items: attend_one(items[0], items[1], items[2], items[3], items[4], items[5], lambdas, head_gain), (queries, cache_keys, cache_values, lengths, new_keys, new_values))
    group_width = attended.shape[1] // N_TP
    summed = jnp.zeros((rows, out_weight.shape[1]), jnp.float32)
    for group in range(N_TP):
        lo_col = group * group_width
        partial_out = jnp.dot(attended[:, lo_col:lo_col + group_width], out_weight[lo_col:lo_col + group_width], preferred_element_type=jnp.float32).astype(jnp.bfloat16)
        summed = summed + lax.optimization_barrier(partial_out).astype(jnp.float32)
    mixed = summed.astype(jnp.bfloat16)
    return (mixed, new_keys, new_values)
```

```python
import functools
import math

import jax
import jax.numpy as jnp
import numpy as np
from jax import lax
from jax.experimental import pallas as pl
from jax.experimental.pallas import tpu as pltpu
from jax.sharding import Mesh
from jax.sharding import PartitionSpec as P

KV = ("kv_0", "kv_1")
MESH = pl.DeviceIdType.MESH

epsilon = 1e-06
rotary_base = 10000.0
masked_score = -1e30
output_scale = 0.2 + 0.6 * math.exp(-0.3)
F32 = jnp.float32
BF16 = jnp.bfloat16


def far_first(n):
    return sorted(range(1, n), key=lambda k: -min(k, n - k))


def near_first(n):
    return sorted(range(1, n), key=lambda k: min(k, n - k))


def kernel(
    nz,
    ny,
    tok_hbm,
    len_hbm,
    wq_hbm,
    wk_hbm,
    wv_hbm,
    qg_hbm,
    kg_hbm,
    lam_hbm,
    hg_hbm,
    ow_hbm,
    ck_hbm,
    cv_hbm,
    freq_hbm,
    mixed_ref,
    nk_ref,
    nv_ref,
    tok,
    wts,
    lens,
    gains,
    lams,
    hgain,
    freq,
    outw,
    ck,
    cv,
    pbuf,
    yrecv,
    zbuf,
    qbuf,
    kvbuf,
    bmsg,
    brecv,
    zw,
    zst,
    attbuf,
    tsend,
    trecv,
    load_sem,
    send_sem,
    recv_sem,
    q_sem,
):
    y = lax.axis_index("kv_1")
    z = lax.axis_index("kv_0")
    core = lax.axis_index("tp")
    positions = ck.shape[1]

    def y_at(k):
        return lax.rem(y + k, ny)

    def z_at(k):
        return lax.rem(z + k, nz)

    barrier = pltpu.get_barrier_semaphore()
    for k in far_first(nz):
        pl.semaphore_signal(barrier, 1, device_id={"kv_0": z_at(k)}, device_id_type=MESH)
    for k in far_first(ny):
        pl.semaphore_signal(barrier, 1, device_id={"kv_1": y_at(k)}, device_id_type=MESH)
    pl.semaphore_signal(barrier, 1, device_id={"tp": 1 - core}, device_id_type=MESH)

    width_q = wq_hbm.shape[1]
    loads = [
        pltpu.make_async_copy(tok_hbm, tok, load_sem.at[0]),
        pltpu.make_async_copy(wq_hbm, wts.at[:, pl.ds(0, width_q)], load_sem.at[1]),
        pltpu.make_async_copy(wk_hbm, wts.at[:, pl.ds(width_q, 128)], load_sem.at[2]),
        pltpu.make_async_copy(wv_hbm, wts.at[:, pl.ds(width_q + 128, 128)], load_sem.at[3]),
        pltpu.make_async_copy(len_hbm, lens, load_sem.at[4]),
        pltpu.make_async_copy(qg_hbm, gains.at[0], load_sem.at[5]),
        pltpu.make_async_copy(kg_hbm, gains.at[1], load_sem.at[6]),
        pltpu.make_async_copy(lam_hbm, lams, load_sem.at[7]),
        pltpu.make_async_copy(hg_hbm, hgain, load_sem.at[8]),
        pltpu.make_async_copy(freq_hbm, freq, load_sem.at[9]),
        pltpu.make_async_copy(ck_hbm, ck, load_sem.at[10]),
        pltpu.make_async_copy(cv_hbm, cv, load_sem.at[11]),
    ]
    heads = width_q // 128
    columns = ow_hbm.shape[0]
    for h in range(heads):
        loads.append(
            pltpu.make_async_copy(
                ow_hbm.at[:, pl.ds(128 * h, 128)],
                outw.at[pl.ds(columns * h, columns)],
                load_sem.at[12 + h],
            )
        )
    for load in loads:
        load.start()

    def send(src, dst, which, axis, target, recv=None):
        copy = pltpu.make_async_remote_copy(
            src_ref=src,
            dst_ref=dst,
            send_sem=send_sem.at[which],
            recv_sem=recv_sem.at[which] if recv is None else recv,
            device_id={axis: target},
            device_id_type=MESH,
        )
        copy.start()

    def all_of(ref, which):
        return pltpu.make_async_remote_copy(
            src_ref=ref,
            dst_ref=ref,
            send_sem=send_sem.at[which],
            recv_sem=recv_sem.at[which],
            device_id={"tp": 1 - core},
            device_id_type=MESH,
        )

    for load in loads[:4]:
        load.wait()
    partial = jnp.dot(tok[...], wts[...], preferred_element_type=F32)
    blocks = heads + 2
    for c in range(blocks):
        pbuf[:, c, :] = partial[:, 128 * c : 128 * (c + 1)]

    pl.semaphore_wait(barrier, (ny - 1) + (nz - 1) + 1)

    for k in far_first(ny):
        send(pbuf.at[y_at(k)], yrecv.at[k - 1], 0, "kv_1", y_at(k))

    for load in loads[4:10]:
        load.wait()
    lane = lax.broadcasted_iota(jnp.int32, (blocks, 128), 1)
    row = lax.broadcasted_iota(jnp.int32, (blocks, 128), 0)
    gain_q = jnp.concatenate([gains[0], gains[0]], axis=1)
    gain_k = jnp.concatenate([gains[1], gains[1]], axis=1)
    gain = jnp.where(row < heads, gain_q, gain_k)
    angle = lens[y].astype(F32) * freq[...]
    cosine = jnp.cos(angle)
    sine = jnp.sin(angle)
    head_row = lax.broadcasted_iota(jnp.int32, (heads, 128), 0)
    lam = jnp.zeros((heads, 128), F32)
    for h in range(heads):
        lam = jnp.where(head_row == h, lams[h], lam)

    all_of(yrecv, 0).wait_recv()
    total = pbuf[y]
    for k in range(ny - 1):
        total = total + yrecv[k]

    zbuf[z] = total
    for k in far_first(nz):
        send(zbuf.at[z], zbuf.at[z], 1, "kv_0", z_at(k))
    all_of(zbuf.at[pl.ds(0, nz - 1)], 1).wait_recv()
    proj = zbuf[0]
    for k in range(1, nz):
        proj = proj + zbuf[k]

    low = lane < 64
    squares = proj * proj
    mean_low = jnp.sum(jnp.where(low, squares, 0.0), axis=1, keepdims=True) / 64
    mean_high = jnp.sum(jnp.where(low, 0.0, squares), axis=1, keepdims=True) / 64
    inverse = jnp.where(low, lax.rsqrt(mean_low + epsilon), lax.rsqrt(mean_high + epsilon))
    normed = proj * inverse * gain
    partner = jnp.where(
        lax.rem(lane, 64) < 32, -pltpu.roll(normed, 96, 1), pltpu.roll(normed, 32, 1)
    )
    rotated = normed * cosine + partner * sine
    qbuf[y] = rotated[:heads].astype(BF16)
    kvbuf[y] = jnp.concatenate([rotated[heads : heads + 1], proj[heads + 1 :]], axis=0)
    for k in far_first(ny):
        send(qbuf.at[y], qbuf.at[y], 2, "kv_1", y_at(k), q_sem.at[k - 1])
    for k in far_first(ny):
        send(kvbuf.at[y], kvbuf.at[y], 3, "kv_1", y_at(k))

    scale = 64 ** (-0.5)
    rows2 = 2 * heads
    wide_lane = lax.broadcasted_iota(jnp.int32, (rows2, 128), 1)
    wide_row = lax.broadcasted_iota(jnp.int32, (rows2, 128), 0)
    eye = wide_lane == wide_row
    half_low = lax.broadcasted_iota(jnp.int32, (heads, 128), 1) < 64
    position_ids = (z * ny + y) * positions + lax.broadcasted_iota(
        jnp.int32, (rows2, positions), 1
    )

    def to_row(column):
        return jnp.sum(jnp.where(eye, column, 0.0), axis=0, keepdims=True)

    def to_column(values):
        return jnp.sum(jnp.where(eye, values, 0.0), axis=1, keepdims=True)

    def two_maps(query):
        return jnp.concatenate(
            [jnp.where(half_low, query, 0.0), jnp.where(half_low, 0.0, query)], axis=0
        )

    def attend(s):
        query = two_maps(qbuf[s].astype(F32)).astype(BF16)
        scores = (
            lax.dot_general(query, ck[s], (((1,), (1,)), ((), ())), preferred_element_type=F32)
            * scale
        )
        valid = position_ids < lens[s]
        highest = jnp.max(jnp.where(valid, scores, masked_score), axis=1, keepdims=True)
        expo = jnp.where(valid, jnp.exp(scores - highest), 0.0)
        count = jnp.sum(expo, axis=1, keepdims=True)
        bmsg[s, pl.ds(0, rows2), :] = jnp.dot(
            expo.astype(BF16), cv[s], preferred_element_type=F32
        )
        bmsg[s, pl.ds(rows2, 2), :] = jnp.concatenate([to_row(highest), to_row(count)], axis=0)

    for load in loads[10:12]:
        load.wait()
    attend(y)
    for k in near_first(ny):
        s = lax.rem(y + ny - k, ny)
        pltpu.make_async_remote_copy(
            src_ref=qbuf.at[s],
            dst_ref=qbuf.at[s],
            send_sem=send_sem.at[2],
            recv_sem=q_sem.at[k - 1],
            device_id={"kv_1": s},
            device_id_type=MESH,
        ).wait_recv()
        attend(s)
        send(bmsg.at[s], brecv.at[k - 1], 4, "kv_1", s)

    own_query = two_maps(qbuf[y].astype(F32))
    own_key = kvbuf[y, pl.ds(0, 1), :].astype(BF16).astype(F32)
    own_value = kvbuf[y, pl.ds(1, 1), :].astype(BF16).astype(F32)
    own_score = to_row(jnp.sum(own_query * own_key, axis=1, keepdims=True) * scale)

    all_of(brecv, 4).wait_recv()
    parts = [bmsg[y]] + [brecv[k] for k in range(ny - 1)]
    highs = [part[rows2 : rows2 + 1] for part in parts]
    high = functools.reduce(jnp.maximum, highs)
    count = jnp.zeros_like(high)
    weighted = jnp.zeros((rows2, 128), F32)
    for part, one in zip(parts, highs):
        factor = jnp.exp(one - high)
        count = count + factor * part[rows2 + 1 :]
        weighted = weighted + to_column(factor) * part[:rows2]
    zw[z] = weighted.astype(BF16)
    zst[z] = jnp.concatenate([high, count], axis=0)
    for k in far_first(nz):
        send(zst.at[z], zst.at[z], 6, "kv_0", z_at(k))
        send(zw.at[z], zw.at[z], 5, "kv_0", z_at(k))
    all_of(zst.at[pl.ds(0, nz - 1)], 6).wait_recv()
    stats = [zst[k] for k in range(nz)]
    high = own_score
    for stat in stats:
        high = jnp.maximum(high, stat[:1])
    own_weight = jnp.exp(own_score - high)
    count = own_weight
    factors = []
    for stat in stats:
        factor = jnp.exp(stat[:1] - high)
        factors.append(factor)
        count = count + factor * stat[1:]
    share = 1.0 / count
    attention = to_column(own_weight * share) * own_value
    columns_of = [to_column(factor * share) for factor in factors]
    all_of(zw.at[pl.ds(0, nz - 1)], 5).wait_recv()
    for k in range(nz):
        attention = attention + columns_of[k] * zw[k].astype(F32)
    gaps = attention[:heads] - lam * attention[heads:]
    mean = jnp.sum(gaps * gaps, axis=1, keepdims=True) / 128
    attended = gaps * lax.rsqrt(mean + epsilon) * hgain[...] * output_scale
    attbuf[y] = attended.astype(BF16)
    for k in far_first(ny):
        send(attbuf.at[y], attbuf.at[y], 7, "kv_1", y_at(k))

    all_of(kvbuf.at[pl.ds(0, ny - 1)], 3).wait_recv()
    for s in range(ny):
        nk_ref[pl.ds(s, 1), :] = kvbuf[s, pl.ds(0, 1), :].astype(BF16)
        nv_ref[pl.ds(s, 1), :] = kvbuf[s, pl.ds(1, 1), :].astype(BF16)
    for load in loads[12:]:
        load.wait()

    all_of(attbuf.at[pl.ds(0, ny - 1)], 7).wait_recv()
    rows = jnp.concatenate([attbuf[s].astype(F32) for s in range(ny)], axis=0).astype(BF16)
    product = lax.dot_general(
        rows, outw[...], (((1,), (1,)), ((), ())), preferred_element_type=F32
    )
    out_row = lax.broadcasted_iota(jnp.int32, product.shape, 0)
    out_lane = lax.broadcasted_iota(jnp.int32, product.shape, 1)
    product = jnp.where(lax.rem(out_row, heads) == out_lane // columns, product, 0.0)
    summed = jnp.sum(product.reshape(ny, heads, 128), axis=1)
    step = columns
    while step < 128:
        summed = summed + pltpu.roll(summed, step, 1)
        step *= 2
    tsend[...] = summed.astype(BF16)
    send(tsend, trecv, 8, "tp", 1 - core)
    all_of(trecv, 8).wait_recv()
    mixed = tsend[...].astype(F32) + trecv[...].astype(F32)
    mixed_ref[...] = mixed[:, :columns].astype(BF16)

    for which, ref in (
        (0, yrecv),
        (1, zbuf.at[pl.ds(0, nz - 1)]),
        (2, qbuf.at[pl.ds(0, ny - 1)]),
        (3, kvbuf.at[pl.ds(0, ny - 1)]),
        (4, brecv),
        (5, zw.at[pl.ds(0, nz - 1)]),
        (6, zst.at[pl.ds(0, nz - 1)]),
        (7, attbuf.at[pl.ds(0, ny - 1)]),
        (8, trecv),
    ):
        all_of(ref, which).wait_send()


def body(
    nz,
    ny,
    tokens,
    lengths,
    query_weight,
    key_weight,
    value_weight,
    query_gain,
    key_gain,
    lambdas,
    head_gain,
    out_weight,
    cache_keys,
    cache_values,
):
    sequences, positions = cache_keys.shape[:2]
    depth, width_q = query_weight.shape
    heads = width_q // 128
    rows2 = 2 * heads
    columns = out_weight.shape[1]
    half = query_gain.shape[0] // 2
    frequency = rotary_base ** (-np.arange(half, dtype=np.float64) / half)
    freq = jnp.asarray(np.tile(frequency, 4).astype(np.float32)[None, :])
    blocks = heads + 2
    any_space = pl.BlockSpec(memory_space=pl.ANY)
    vmem = pl.BlockSpec(memory_space=pltpu.VMEM)
    mixed, new_keys, new_values = pl.pallas_call(
        functools.partial(kernel, nz, ny),
        name="decode_step",
        out_shape=(
            jax.ShapeDtypeStruct((sequences, columns), BF16),
            jax.ShapeDtypeStruct((sequences, 128), BF16),
            jax.ShapeDtypeStruct((sequences, 128), BF16),
        ),
        in_specs=[any_space] * 13,
        out_specs=(vmem, vmem, vmem),
        scratch_shapes=[
            pltpu.VMEM((sequences, depth), BF16),
            pltpu.VMEM((depth, width_q + 256), BF16),
            pltpu.SMEM((sequences,), jnp.int32),
            pltpu.VMEM((2, 1, 64), F32),
            pltpu.SMEM((heads,), F32),
            pltpu.VMEM((1, 128), F32),
            pltpu.VMEM((1, 128), F32),
            pltpu.VMEM((heads * columns, 128), BF16),
            pltpu.VMEM((sequences, positions, 128), BF16),
            pltpu.VMEM((sequences, positions, 128), BF16),
            pltpu.VMEM((sequences, blocks, 128), F32),
            pltpu.VMEM((ny - 1, blocks, 128), F32),
            pltpu.VMEM((nz, blocks, 128), F32),
            pltpu.VMEM((ny, heads, 128), BF16),
            pltpu.VMEM((ny, 2, 128), F32),
            pltpu.VMEM((ny, rows2 + 2, 128), F32),
            pltpu.VMEM((ny - 1, rows2 + 2, 128), F32),
            pltpu.VMEM((nz, rows2, 128), BF16),
            pltpu.VMEM((nz, 2, 128), F32),
            pltpu.VMEM((ny, heads, 128), BF16),
            pltpu.VMEM((sequences, 128), BF16),
            pltpu.VMEM((sequences, 128), BF16),
            pltpu.SemaphoreType.DMA((12 + heads,)),
            pltpu.SemaphoreType.DMA((9,)),
            pltpu.SemaphoreType.DMA((9,)),
            pltpu.SemaphoreType.DMA((ny - 1,)),
        ],
        compiler_params=pltpu.CompilerParams(collective_id=0, has_side_effects=True),
    )(
        tokens,
        lengths,
        query_weight,
        key_weight,
        value_weight,
        query_gain.reshape(1, -1),
        key_gain.reshape(1, -1),
        lambdas,
        head_gain.reshape(1, -1),
        out_weight.T,
        cache_keys.reshape(sequences, positions, 128),
        cache_values.reshape(sequences, positions, 128),
        freq,
    )
    return (
        mixed,
        new_keys.reshape(sequences, 1, 128),
        new_values.reshape(sequences, 1, 128),
    )


def solution(mesh):
    ny = 8
    nz = mesh.shape["kv"] // ny
    finer = Mesh(
        mesh.devices.reshape(mesh.shape["dp"], nz, ny, mesh.shape["tp"]),
        ("dp", "kv_0", "kv_1", "tp"),
    )
    in_specs = (
        P("dp", KV),
        P("dp"),
        P(KV, "tp"),
        P(KV, "tp"),
        P(KV, "tp"),
        P(),
        P(),
        P("tp"),
        P(),
        P("tp", KV),
        P("dp", KV, "tp", None),
        P("dp", KV, "tp", None),
    )
    out_specs = (P("dp", KV), P("dp", "tp", None), P("dp", "tp", None))
    return jax.shard_map(
        functools.partial(body, nz, ny),
        mesh=finer,
        in_specs=in_specs,
        out_specs=out_specs,
        check_vma=False,
    )
```

```python
import functools
import math

import jax
import jax.numpy as jnp
import numpy as np
from jax import lax
from jax.experimental import pallas as pl
from jax.experimental.pallas import tpu as pltpu
from jax.sharding import Mesh
from jax.sharding import PartitionSpec as P

KV = ("kv_0", "kv_1")
MESH = pl.DeviceIdType.MESH

epsilon = 1e-06
rotary_base = 10000.0
masked_score = -1e30
output_scale = 0.2 + 0.6 * math.exp(-0.3)
F32 = jnp.float32
BF16 = jnp.bfloat16


def far_first(n):
    return sorted(range(1, n), key=lambda k: -min(k, n - k))


def near_first(n):
    return sorted(range(1, n), key=lambda k: min(k, n - k))


def kernel(
    nz,
    ny,
    tok_hbm,
    len_hbm,
    wq_hbm,
    wk_hbm,
    wv_hbm,
    qg_hbm,
    kg_hbm,
    lam_hbm,
    hg_hbm,
    ow_hbm,
    ck_hbm,
    cv_hbm,
    freq_hbm,
    out_ref,
    tok,
    wts,
    lens,
    gains,
    lams,
    hgain,
    freq,
    outw,
    ck,
    cv,
    pbuf,
    yrecv,
    zbuf,
    qbuf,
    kvbuf,
    bmsg,
    brecv,
    zw,
    zst,
    attbuf,
    load_sem,
    send_sem,
    recv_sem,
    q_sem,
    reach_sem,
):
    y = lax.axis_index("kv_1")
    z = lax.axis_index("kv_0")
    core = lax.axis_index("tp")
    positions = ck.shape[1]

    def y_at(k):
        return lax.rem(y + k, ny)

    def z_at(k):
        return lax.rem(z + k, nz)

    barrier = pltpu.get_barrier_semaphore()
    for k in far_first(ny):
        pl.semaphore_signal(barrier, 1, device_id={"kv_1": y_at(k)}, device_id_type=MESH)
        pl.semaphore_signal(
            barrier, 1, device_id={"kv_1": y_at(k), "tp": 1 - core}, device_id_type=MESH
        )
    for k in (1, nz - 1):
        pl.semaphore_signal(barrier, 1, device_id={"kv_0": z_at(k)}, device_id_type=MESH)
    pl.semaphore_signal(barrier, 1, device_id={"tp": 1 - core}, device_id_type=MESH)

    width_q = wq_hbm.shape[1]
    loads = [
        pltpu.make_async_copy(tok_hbm, tok, load_sem.at[0]),
        pltpu.make_async_copy(wq_hbm, wts.at[:, pl.ds(0, width_q)], load_sem.at[1]),
        pltpu.make_async_copy(wk_hbm, wts.at[:, pl.ds(width_q, 128)], load_sem.at[2]),
        pltpu.make_async_copy(wv_hbm, wts.at[:, pl.ds(width_q + 128, 128)], load_sem.at[3]),
        pltpu.make_async_copy(len_hbm, lens, load_sem.at[4]),
        pltpu.make_async_copy(qg_hbm, gains.at[0], load_sem.at[5]),
        pltpu.make_async_copy(kg_hbm, gains.at[1], load_sem.at[6]),
        pltpu.make_async_copy(lam_hbm, lams, load_sem.at[7]),
        pltpu.make_async_copy(hg_hbm, hgain, load_sem.at[8]),
        pltpu.make_async_copy(freq_hbm, freq, load_sem.at[9]),
        pltpu.make_async_copy(ck_hbm, ck, load_sem.at[10]),
        pltpu.make_async_copy(cv_hbm, cv, load_sem.at[11]),
    ]
    heads = width_q // 128
    columns = ow_hbm.shape[0]
    for h in range(heads):
        loads.append(
            pltpu.make_async_copy(
                ow_hbm.at[:, pl.ds(128 * h, 128)],
                outw.at[core, pl.ds(columns * h, columns)],
                load_sem.at[12 + h],
            )
        )
    for load in loads:
        load.start()

    def tell(round_number, reach):
        if round_number > 0:
            pl.semaphore_wait(reach_sem.at[round_number - 1], 2)
        for k in (reach, nz - reach):
            pl.semaphore_signal(
                reach_sem.at[round_number],
                1,
                device_id={"kv_0": z_at(k)},
                device_id_type=MESH,
            )

    def send(src, dst, which, target, recv=None):
        copy = pltpu.make_async_remote_copy(
            src_ref=src,
            dst_ref=dst,
            send_sem=send_sem.at[which],
            recv_sem=recv_sem.at[which] if recv is None else recv,
            device_id=target,
            device_id_type=MESH,
        )
        copy.start()

    def all_of(ref, which):
        return pltpu.make_async_remote_copy(
            src_ref=ref,
            dst_ref=ref,
            send_sem=send_sem.at[which],
            recv_sem=recv_sem.at[which],
            device_id={"tp": 1 - core},
            device_id_type=MESH,
        )

    for load in loads[:4]:
        load.wait()
    partial = jnp.dot(tok[...], wts[...], preferred_element_type=F32)
    blocks = heads + 2
    for c in range(blocks):
        pbuf[:, c, :] = partial[:, 128 * c : 128 * (c + 1)]

    pl.semaphore_wait(barrier, 2 * (ny - 1) + 2 + 1)

    for k in far_first(ny):
        send(pbuf.at[y_at(k)], yrecv.at[k - 1], 0, {"kv_1": y_at(k)})
    if nz > 2:
        tell(0, 1)

    for load in loads[4:10]:
        load.wait()
    lane = lax.broadcasted_iota(jnp.int32, (blocks, 128), 1)
    row = lax.broadcasted_iota(jnp.int32, (blocks, 128), 0)
    gain_q = jnp.concatenate([gains[0], gains[0]], axis=1)
    gain_k = jnp.concatenate([gains[1], gains[1]], axis=1)
    gain = jnp.where(row < heads, gain_q, gain_k)
    angle = lens[y].astype(F32) * freq[...]
    cosine = jnp.cos(angle)
    sine = jnp.sin(angle)
    head_row = lax.broadcasted_iota(jnp.int32, (heads, 128), 0)
    lam = jnp.zeros((heads, 128), F32)
    for h in range(heads):
        lam = jnp.where(head_row == h, lams[h], lam)

    reach, round_number = 2, 1
    while reach < nz // 2:
        tell(round_number, reach)
        reach, round_number = 2 * reach, round_number + 1
    if nz > 2:
        pl.semaphore_wait(reach_sem.at[round_number - 1], 2)

    for load in loads[12:]:
        load.wait()
    send(outw.at[core], outw.at[core], 8, {"tp": 1 - core})

    all_of(yrecv, 0).wait_recv()
    total = pbuf[y]
    for k in range(ny - 1):
        total = total + yrecv[k]

    zbuf[z] = total
    for k in far_first(nz):
        send(zbuf.at[z], zbuf.at[z], 1, {"kv_0": z_at(k)})
    all_of(zbuf.at[pl.ds(0, nz - 1)], 1).wait_recv()
    proj = zbuf[0]
    for k in range(1, nz):
        proj = proj + zbuf[k]

    low = lane < 64
    squares = proj * proj
    mean_low = jnp.sum(jnp.where(low, squares, 0.0), axis=1, keepdims=True) / 64
    mean_high = jnp.sum(jnp.where(low, 0.0, squares), axis=1, keepdims=True) / 64
    inverse = jnp.where(low, lax.rsqrt(mean_low + epsilon), lax.rsqrt(mean_high + epsilon))
    normed = proj * inverse * gain
    partner = jnp.where(
        lax.rem(lane, 64) < 32, -pltpu.roll(normed, 96, 1), pltpu.roll(normed, 32, 1)
    )
    rotated = normed * cosine + partner * sine
    qbuf[y] = rotated[:heads].astype(BF16)
    kvbuf[y] = jnp.concatenate([rotated[heads : heads + 1], proj[heads + 1 :]], axis=0)
    for k in far_first(ny):
        send(qbuf.at[y], qbuf.at[y], 2, {"kv_1": y_at(k)}, q_sem.at[k - 1])
    for k in far_first(ny):
        send(kvbuf.at[y], kvbuf.at[y], 3, {"kv_1": y_at(k)})

    scale = 64 ** (-0.5)
    rows2 = 2 * heads
    wide_lane = lax.broadcasted_iota(jnp.int32, (rows2, 128), 1)
    wide_row = lax.broadcasted_iota(jnp.int32, (rows2, 128), 0)
    eye = wide_lane == wide_row
    half_low = lax.broadcasted_iota(jnp.int32, (heads, 128), 1) < 64
    position_ids = (z * ny + y) * positions + lax.broadcasted_iota(
        jnp.int32, (rows2, positions), 1
    )

    def to_row(column):
        return jnp.sum(jnp.where(eye, column, 0.0), axis=0, keepdims=True)

    def to_column(values):
        return jnp.sum(jnp.where(eye, values, 0.0), axis=1, keepdims=True)

    def two_maps(query):
        return jnp.concatenate(
            [jnp.where(half_low, query, 0.0), jnp.where(half_low, 0.0, query)], axis=0
        )

    def attend(s):
        query = two_maps(qbuf[s].astype(F32)).astype(BF16)
        scores = (
            lax.dot_general(query, ck[s], (((1,), (1,)), ((), ())), preferred_element_type=F32)
            * scale
        )
        valid = position_ids < lens[s]
        highest = jnp.max(jnp.where(valid, scores, masked_score), axis=1, keepdims=True)
        expo = jnp.where(valid, jnp.exp(scores - highest), 0.0)
        count = jnp.sum(expo, axis=1, keepdims=True)
        bmsg[s, pl.ds(0, rows2), :] = jnp.dot(
            expo.astype(BF16), cv[s], preferred_element_type=F32
        )
        bmsg[s, pl.ds(rows2, 2), :] = jnp.concatenate([to_row(highest), to_row(count)], axis=0)

    for load in loads[10:12]:
        load.wait()
    attend(y)
    for k in near_first(ny):
        s = lax.rem(y + ny - k, ny)
        pltpu.make_async_remote_copy(
            src_ref=qbuf.at[s],
            dst_ref=qbuf.at[s],
            send_sem=send_sem.at[2],
            recv_sem=q_sem.at[k - 1],
            device_id={"kv_1": s},
            device_id_type=MESH,
        ).wait_recv()
        attend(s)
        send(bmsg.at[s], brecv.at[k - 1], 4, {"kv_1": s})

    own_query = two_maps(qbuf[y].astype(F32))
    own_key = kvbuf[y, pl.ds(0, 1), :].astype(BF16).astype(F32)
    own_value = kvbuf[y, pl.ds(1, 1), :].astype(BF16).astype(F32)
    own_score = to_row(jnp.sum(own_query * own_key, axis=1, keepdims=True) * scale)

    all_of(brecv, 4).wait_recv()
    parts = [bmsg[y]] + [brecv[k] for k in range(ny - 1)]
    highs = [part[rows2 : rows2 + 1] for part in parts]
    high = functools.reduce(jnp.maximum, highs)
    count = jnp.zeros_like(high)
    weighted = jnp.zeros((rows2, 128), F32)
    for part, one in zip(parts, highs):
        factor = jnp.exp(one - high)
        count = count + factor * part[rows2 + 1 :]
        weighted = weighted + to_column(factor) * part[:rows2]
    zw[z] = weighted.astype(BF16)
    zst[z] = jnp.concatenate([high, count], axis=0)
    for k in far_first(nz):
        send(zst.at[z], zst.at[z], 6, {"kv_0": z_at(k)})
        send(zw.at[z], zw.at[z], 5, {"kv_0": z_at(k)})
    all_of(zst.at[pl.ds(0, nz - 1)], 6).wait_recv()
    stats = [zst[k] for k in range(nz)]
    high = own_score
    for stat in stats:
        high = jnp.maximum(high, stat[:1])
    own_weight = jnp.exp(own_score - high)
    count = own_weight
    factors = []
    for stat in stats:
        factor = jnp.exp(stat[:1] - high)
        factors.append(factor)
        count = count + factor * stat[1:]
    share = 1.0 / count
    attention = to_column(own_weight * share) * own_value
    columns_of = [to_column(factor * share) for factor in factors]
    all_of(zw.at[pl.ds(0, nz - 1)], 5).wait_recv()
    for k in range(nz):
        attention = attention + columns_of[k] * zw[k].astype(F32)
    gaps = attention[:heads] - lam * attention[heads:]
    mean = jnp.sum(gaps * gaps, axis=1, keepdims=True) / 128
    attended = gaps * lax.rsqrt(mean + epsilon) * hgain[...] * output_scale
    attbuf[core * ny + y] = attended.astype(BF16)
    mine = attbuf.at[core * ny + y]
    for k in far_first(ny):
        send(mine, mine, 7, {"kv_1": y_at(k)})
        send(mine, mine, 7, {"kv_1": y_at(k), "tp": 1 - core})
    send(mine, mine, 7, {"tp": 1 - core})

    all_of(kvbuf.at[pl.ds(0, ny - 1)], 3).wait_recv()
    for s in range(ny):
        out_ref[pl.ds(s, 1), pl.ds(128, 128)] = kvbuf[s, pl.ds(0, 1), :]
        out_ref[pl.ds(s, 1), pl.ds(256, 128)] = kvbuf[s, pl.ds(1, 1), :]
    all_of(outw.at[0], 8).wait_recv()

    all_of(attbuf.at[pl.ds(0, 2 * ny - 1)], 7).wait_recv()
    mixed = jnp.zeros((ny, 128), F32)
    for group in range(2):
        rows = jnp.concatenate(
            [attbuf[group * ny + s].astype(F32) for s in range(ny)], axis=0
        ).astype(BF16)
        product = lax.dot_general(
            rows, outw[group], (((1,), (1,)), ((), ())), preferred_element_type=F32
        )
        out_row = lax.broadcasted_iota(jnp.int32, product.shape, 0)
        out_lane = lax.broadcasted_iota(jnp.int32, product.shape, 1)
        product = jnp.where(lax.rem(out_row, heads) == out_lane // columns, product, 0.0)
        summed = jnp.sum(product.reshape(ny, heads, 128), axis=1)
        step = columns
        while step < 128:
            summed = summed + pltpu.roll(summed, step, 1)
            step *= 2
        mixed = mixed + summed.astype(BF16).astype(F32)
    out_ref[:, pl.ds(0, 128)] = mixed

    for which, ref in (
        (0, yrecv),
        (1, zbuf.at[pl.ds(0, nz - 1)]),
        (2, qbuf.at[pl.ds(0, ny - 1)]),
        (3, kvbuf.at[pl.ds(0, ny - 1)]),
        (4, brecv),
        (5, zw.at[pl.ds(0, nz - 1)]),
        (6, zst.at[pl.ds(0, nz - 1)]),
        (7, attbuf.at[pl.ds(0, 2 * ny - 1)]),
        (8, outw.at[0]),
    ):
        all_of(ref, which).wait_send()


def cut(x_ref, mixed_ref, nk_ref, nv_ref):
    mixed_ref[...] = x_ref[:, : mixed_ref.shape[1]].astype(BF16)
    nk_ref[...] = x_ref[:, 128:256].astype(BF16)
    nv_ref[...] = x_ref[:, 256:].astype(BF16)


def body(
    nz,
    ny,
    tokens,
    lengths,
    query_weight,
    key_weight,
    value_weight,
    query_gain,
    key_gain,
    lambdas,
    head_gain,
    out_weight,
    cache_keys,
    cache_values,
):
    sequences, positions = cache_keys.shape[:2]
    depth, width_q = query_weight.shape
    heads = width_q // 128
    rows2 = 2 * heads
    columns = out_weight.shape[1]
    half = query_gain.shape[0] // 2
    frequency = rotary_base ** (-np.arange(half, dtype=np.float64) / half)
    freq = jnp.asarray(np.tile(frequency, 4).astype(np.float32)[None, :])
    blocks = heads + 2
    any_space = pl.BlockSpec(memory_space=pl.ANY)
    vmem = pl.BlockSpec(memory_space=pltpu.VMEM)
    out = pl.pallas_call(
        functools.partial(kernel, nz, ny),
        name="decode_step",
        out_shape=pltpu.VMEM((sequences, 384), F32),
        in_specs=[any_space] * 13,
        out_specs=vmem,
        scratch_shapes=[
            pltpu.VMEM((sequences, depth), BF16),
            pltpu.VMEM((depth, width_q + 256), BF16),
            pltpu.SMEM((sequences,), jnp.int32),
            pltpu.VMEM((2, 1, 64), F32),
            pltpu.SMEM((heads,), F32),
            pltpu.VMEM((1, 128), F32),
            pltpu.VMEM((1, 128), F32),
            pltpu.VMEM((2, heads * columns, 128), BF16),
            pltpu.VMEM((sequences, positions, 128), BF16),
            pltpu.VMEM((sequences, positions, 128), BF16),
            pltpu.VMEM((sequences, blocks, 128), F32),
            pltpu.VMEM((ny - 1, blocks, 128), F32),
            pltpu.VMEM((nz, blocks, 128), F32),
            pltpu.VMEM((ny, heads, 128), BF16),
            pltpu.VMEM((ny, 2, 128), F32),
            pltpu.VMEM((ny, rows2 + 2, 128), F32),
            pltpu.VMEM((ny - 1, rows2 + 2, 128), F32),
            pltpu.VMEM((nz, rows2, 128), BF16),
            pltpu.VMEM((nz, 2, 128), F32),
            pltpu.VMEM((2 * ny, heads, 128), BF16),
            pltpu.SemaphoreType.DMA((12 + heads,)),
            pltpu.SemaphoreType.DMA((9,)),
            pltpu.SemaphoreType.DMA((9,)),
            pltpu.SemaphoreType.DMA((ny - 1,)),
            pltpu.SemaphoreType.REGULAR((4,)),
        ],
        compiler_params=pltpu.CompilerParams(collective_id=0, has_side_effects=True),
    )(
        tokens,
        lengths,
        query_weight,
        key_weight,
        value_weight,
        query_gain.reshape(1, -1),
        key_gain.reshape(1, -1),
        lambdas,
        head_gain.reshape(1, -1),
        out_weight.T,
        cache_keys.reshape(sequences, positions, 128),
        cache_values.reshape(sequences, positions, 128),
        freq,
    )
    mixed, new_keys, new_values = pl.pallas_call(
        cut,
        name="cut",
        out_shape=(
            jax.ShapeDtypeStruct((sequences, columns), BF16),
            jax.ShapeDtypeStruct((sequences, 128), BF16),
            jax.ShapeDtypeStruct((sequences, 128), BF16),
        ),
        in_specs=[vmem],
        out_specs=(vmem, vmem, vmem),
    )(pltpu.with_memory_space_constraint(out, pltpu.VMEM))
    return (
        mixed,
        new_keys.reshape(sequences, 1, 128),
        new_values.reshape(sequences, 1, 128),
    )


def solution(mesh):
    ny = 8
    nz = mesh.shape["kv"] // ny
    finer = Mesh(
        mesh.devices.reshape(mesh.shape["dp"], nz, ny, mesh.shape["tp"]),
        ("dp", "kv_0", "kv_1", "tp"),
    )
    in_specs = (
        P("dp", KV),
        P("dp"),
        P(KV, "tp"),
        P(KV, "tp"),
        P(KV, "tp"),
        P(),
        P(),
        P("tp"),
        P(),
        P("tp", KV),
        P("dp", KV, "tp", None),
        P("dp", KV, "tp", None),
    )
    out_specs = (P("dp", KV), P("dp", "tp", None), P("dp", "tp", None))
    return jax.shard_map(
        functools.partial(body, nz, ny),
        mesh=finer,
        in_specs=in_specs,
        out_specs=out_specs,
        check_vma=False,
    )
```

```python
import functools
import math

import jax
import jax.numpy as jnp
import numpy as np
from jax import lax
from jax.experimental import pallas as pl
from jax.experimental.pallas import tpu as pltpu
from jax.sharding import Mesh
from jax.sharding import PartitionSpec as P

KV = ("kv_0", "kv_1")
MESH = pl.DeviceIdType.MESH

epsilon = 1e-06
rotary_base = 10000.0
masked_score = -1e30
output_scale = 0.2 + 0.6 * math.exp(-0.3)
F32 = jnp.float32
BF16 = jnp.bfloat16


def far_first(n):
    return sorted(range(1, n), key=lambda k: -min(k, n - k))


STAY = 2


def near_first(n):
    return [k for k in sorted(range(1, n), key=lambda k: min(k, n - k)) if min(k, n - k) <= STAY]


def moved(n):
    return [k for k in far_first(n) if min(k, n - k) > STAY]


def kernel(
    nz,
    ny,
    tok_hbm,
    len_hbm,
    wq_hbm,
    wk_hbm,
    wv_hbm,
    qg_hbm,
    kg_hbm,
    lam_hbm,
    hg_hbm,
    ow_hbm,
    ck_hbm,
    cv_hbm,
    freq_hbm,
    out_ref,
    tok,
    wts,
    lens,
    gains,
    lams,
    hgain,
    freq,
    outw,
    ck,
    cv,
    pbuf,
    yrecv,
    zsend,
    zbuf,
    qbuf,
    kvbuf,
    kfar,
    vfar,
    bmsg,
    brecv,
    zwsend,
    zstsend,
    zw,
    zst,
    attbuf,
    load_sem,
    send_sem,
    recv_sem,
    q_sem,
    reach_sem,
):
    y = lax.axis_index("kv_1")
    z = lax.axis_index("kv_0")
    core = lax.axis_index("tp")
    other = 1 - core
    positions = ck.shape[1]

    def y_at(k):
        return lax.rem(y + k, ny)

    def z_at(k):
        return lax.rem(z + k, nz)

    barrier = pltpu.get_barrier_semaphore()
    for k in far_first(ny):
        pl.semaphore_signal(barrier, 1, device_id={"kv_1": y_at(k)}, device_id_type=MESH)
        pl.semaphore_signal(
            barrier, 1, device_id={"kv_1": y_at(k), "tp": other}, device_id_type=MESH
        )
    for k in (1, nz - 1):
        pl.semaphore_signal(barrier, 1, device_id={"kv_0": z_at(k)}, device_id_type=MESH)
        pl.semaphore_signal(
            barrier, 1, device_id={"kv_0": z_at(k), "tp": other}, device_id_type=MESH
        )
    pl.semaphore_signal(barrier, 1, device_id={"tp": other}, device_id_type=MESH)

    width_q = wq_hbm.shape[1]
    loads = [
        pltpu.make_async_copy(tok_hbm, tok, load_sem.at[0]),
        pltpu.make_async_copy(wq_hbm, wts.at[:, pl.ds(0, width_q)], load_sem.at[1]),
        pltpu.make_async_copy(wk_hbm, wts.at[:, pl.ds(width_q, 128)], load_sem.at[2]),
        pltpu.make_async_copy(wv_hbm, wts.at[:, pl.ds(width_q + 128, 128)], load_sem.at[3]),
        pltpu.make_async_copy(len_hbm, lens, load_sem.at[4]),
        pltpu.make_async_copy(qg_hbm, gains.at[0], load_sem.at[5]),
        pltpu.make_async_copy(kg_hbm, gains.at[1], load_sem.at[6]),
        pltpu.make_async_copy(lam_hbm, lams, load_sem.at[7]),
        pltpu.make_async_copy(hg_hbm, hgain, load_sem.at[8]),
        pltpu.make_async_copy(freq_hbm, freq, load_sem.at[9]),
        pltpu.make_async_copy(ck_hbm, ck, load_sem.at[10]),
        pltpu.make_async_copy(cv_hbm, cv, load_sem.at[11]),
    ]
    heads = width_q // 128
    columns = ow_hbm.shape[0]
    for h in range(heads):
        loads.append(
            pltpu.make_async_copy(
                ow_hbm.at[:, pl.ds(128 * h, 128)],
                outw.at[core, pl.ds(columns * h, columns)],
                load_sem.at[12 + h],
            )
        )
    for load in loads:
        load.start()

    def tell(round_number, reach):
        if round_number > 0:
            pl.semaphore_wait(reach_sem.at[round_number - 1], 2)
        for k in (reach, nz - reach):
            pl.semaphore_signal(
                reach_sem.at[round_number],
                1,
                device_id={"kv_0": z_at(k)},
                device_id_type=MESH,
            )

    def send(src, dst, which, target, recv=None):
        copy = pltpu.make_async_remote_copy(
            src_ref=src,
            dst_ref=dst,
            send_sem=send_sem.at[which],
            recv_sem=recv_sem.at[which] if recv is None else recv,
            device_id=target,
            device_id_type=MESH,
        )
        copy.start()

    def all_of(ref, which):
        return pltpu.make_async_remote_copy(
            src_ref=ref,
            dst_ref=ref,
            send_sem=send_sem.at[which],
            recv_sem=recv_sem.at[which],
            device_id={"tp": other},
            device_id_type=MESH,
        )

    for load in loads[:4]:
        load.wait()
    partial = jnp.dot(tok[...], wts[...], preferred_element_type=F32)
    blocks = heads + 2
    for c in range(blocks):
        pbuf[:, c, :] = partial[:, 128 * c : 128 * (c + 1)]

    pl.semaphore_wait(barrier, 2 * (ny - 1) + 4 + 1)

    for k in far_first(ny):
        send(pbuf.at[y_at(k)], yrecv.at[k], 0, {"kv_1": y_at(k), "tp": other})
    send(pbuf.at[y], yrecv.at[0], 0, {"tp": other})
    if nz > 2:
        tell(0, 1)
    for i, k in enumerate(moved(ny)):
        send(ck_hbm.at[y_at(k)], kfar.at[i], 9, {"kv_1": y_at(k)})
    for i, k in enumerate(moved(ny)):
        send(cv_hbm.at[y_at(k)], vfar.at[i], 10, {"kv_1": y_at(k)})

    for load in loads[4:10]:
        load.wait()
    lane = lax.broadcasted_iota(jnp.int32, (blocks, 128), 1)
    row = lax.broadcasted_iota(jnp.int32, (blocks, 128), 0)
    gain_q = jnp.concatenate([gains[0], gains[0]], axis=1)
    gain_k = jnp.concatenate([gains[1], gains[1]], axis=1)
    gain = jnp.where(row < heads, gain_q, gain_k)
    angle = lens[y].astype(F32) * freq[...]
    cosine = jnp.cos(angle)
    sine = jnp.sin(angle)
    head_row = lax.broadcasted_iota(jnp.int32, (heads, 128), 0)
    lam = jnp.zeros((heads, 128), F32)
    for h in range(heads):
        lam = jnp.where(head_row == h, lams[h], lam)

    reach, round_number = 2, 1
    while reach < nz // 2:
        tell(round_number, reach)
        reach, round_number = 2 * reach, round_number + 1
    if nz > 2:
        pl.semaphore_wait(reach_sem.at[round_number - 1], 2)

    for load in loads[12:]:
        load.wait()
    send(outw.at[core], outw.at[core], 8, {"tp": other})

    all_of(yrecv, 0).wait_recv()
    total = yrecv[0]
    for k in range(1, ny):
        total = total + yrecv[k]

    zsend[...] = total
    for k in far_first(nz):
        send(zsend, zbuf.at[z], 1, {"kv_0": z_at(k), "tp": other})
    send(zsend, zbuf.at[z], 1, {"tp": other})
    all_of(zbuf, 1).wait_recv()
    proj = zbuf[0]
    for k in range(1, nz):
        proj = proj + zbuf[k]

    low = lane < 64
    squares = proj * proj
    mean_low = jnp.sum(jnp.where(low, squares, 0.0), axis=1, keepdims=True) / 64
    mean_high = jnp.sum(jnp.where(low, 0.0, squares), axis=1, keepdims=True) / 64
    inverse = jnp.where(low, lax.rsqrt(mean_low + epsilon), lax.rsqrt(mean_high + epsilon))
    normed = proj * inverse * gain
    partner = jnp.where(
        lax.rem(lane, 64) < 32, -pltpu.roll(normed, 96, 1), pltpu.roll(normed, 32, 1)
    )
    rotated = normed * cosine + partner * sine
    qbuf[y] = rotated[:heads].astype(BF16)
    kvbuf[y] = jnp.concatenate([rotated[heads : heads + 1], proj[heads + 1 :]], axis=0)
    near = near_first(ny)
    for k in reversed(near):
        send(qbuf.at[y], qbuf.at[y], 2, {"kv_1": y_at(k)}, q_sem.at[k - 1])
    for k in far_first(ny):
        send(kvbuf.at[y], kvbuf.at[y], 3, {"kv_1": y_at(k)})

    scale = 64 ** (-0.5)
    rows2 = 2 * heads
    wide_lane = lax.broadcasted_iota(jnp.int32, (rows2, 128), 1)
    wide_row = lax.broadcasted_iota(jnp.int32, (rows2, 128), 0)
    eye = wide_lane == wide_row
    half_low = lax.broadcasted_iota(jnp.int32, (heads, 128), 1) < 64
    position = lax.broadcasted_iota(jnp.int32, (rows2, positions), 1)

    def to_row(column):
        return jnp.sum(jnp.where(eye, column, 0.0), axis=0, keepdims=True)

    def to_column(values):
        return jnp.sum(jnp.where(eye, values, 0.0), axis=1, keepdims=True)

    def two_maps(query):
        return jnp.concatenate(
            [jnp.where(half_low, query, 0.0), jnp.where(half_low, 0.0, query)], axis=0
        )

    def attend(s, blocks, out):
        query = two_maps(qbuf[s].astype(F32)).astype(BF16)
        scores, valid = [], []
        for keys, _, where in blocks:
            scores.append(
                lax.dot_general(query, keys, (((1,), (1,)), ((), ())), preferred_element_type=F32)
                * scale
            )
            valid.append(position < lens[s] - (z * ny + where) * positions)
        highest = functools.reduce(
            jnp.maximum, [jnp.where(v, x, masked_score) for v, x in zip(valid, scores)]
        )
        highest = jnp.max(highest, axis=1, keepdims=True)
        expo = [jnp.where(v, jnp.exp(x - highest), 0.0) for v, x in zip(valid, scores)]
        count = jnp.sum(functools.reduce(jnp.add, expo), axis=1, keepdims=True)
        bmsg[out, pl.ds(0, rows2), :] = functools.reduce(
            jnp.add,
            [
                jnp.dot(e.astype(BF16), values, preferred_element_type=F32)
                for e, (_, values, _) in zip(expo, blocks)
            ],
        )
        bmsg[out, pl.ds(rows2, 2), :] = jnp.concatenate([to_row(highest), to_row(count)], axis=0)

    for load in loads[10:12]:
        load.wait()
    for k in near:
        s = lax.rem(y + ny - k, ny)
        pltpu.make_async_remote_copy(
            src_ref=qbuf.at[s],
            dst_ref=qbuf.at[s],
            send_sem=send_sem.at[2],
            recv_sem=q_sem.at[k - 1],
            device_id={"kv_1": s},
            device_id_type=MESH,
        ).wait_recv()
        attend(s, [(ck[s], cv[s], y)], s)
        send(bmsg.at[s], brecv.at[near.index(k)], 4, {"kv_1": s, "tp": other})

    all_of(kfar, 9).wait_recv()
    all_of(vfar, 10).wait_recv()
    attend(
        y,
        [(ck[y], cv[y], y)]
        + [(kfar[i], vfar[i], lax.rem(y + ny - k, ny)) for i, k in enumerate(moved(ny))],
        y,
    )

    send(bmsg.at[y], brecv.at[len(near)], 4, {"tp": other})

    own_query = two_maps(qbuf[y].astype(F32))
    own_key = kvbuf[y, pl.ds(0, 1), :].astype(BF16).astype(F32)
    own_value = kvbuf[y, pl.ds(1, 1), :].astype(BF16).astype(F32)
    own_score = to_row(jnp.sum(own_query * own_key, axis=1, keepdims=True) * scale)

    all_of(brecv, 4).wait_recv()
    parts = [brecv[i] for i in range(len(near) + 1)]
    highs = [part[rows2 : rows2 + 1] for part in parts]
    high = functools.reduce(jnp.maximum, highs)
    count = jnp.zeros_like(high)
    weighted = jnp.zeros((rows2, 128), F32)
    for part, one in zip(parts, highs):
        factor = jnp.exp(one - high)
        count = count + factor * part[rows2 + 1 :]
        weighted = weighted + to_column(factor) * part[:rows2]
    zwsend[...] = weighted.astype(BF16)
    zstsend[...] = jnp.concatenate([high, count], axis=0)
    for k in far_first(nz):
        send(zstsend, zst.at[z], 6, {"kv_0": z_at(k), "tp": other})
        send(zwsend, zw.at[z], 5, {"kv_0": z_at(k), "tp": other})
    send(zstsend, zst.at[z], 6, {"tp": other})
    send(zwsend, zw.at[z], 5, {"tp": other})
    all_of(zst, 6).wait_recv()
    stats = [zst[k] for k in range(nz)]
    high = own_score
    for stat in stats:
        high = jnp.maximum(high, stat[:1])
    own_weight = jnp.exp(own_score - high)
    count = own_weight
    factors = []
    for stat in stats:
        factor = jnp.exp(stat[:1] - high)
        factors.append(factor)
        count = count + factor * stat[1:]
    share = 1.0 / count
    attention = to_column(own_weight * share) * own_value
    columns_of = [to_column(factor * share) for factor in factors]
    all_of(zw, 5).wait_recv()
    for k in range(nz):
        attention = attention + columns_of[k] * zw[k].astype(F32)
    gaps = attention[:heads] - lam * attention[heads:]
    mean = jnp.sum(gaps * gaps, axis=1, keepdims=True) / 128
    attended = gaps * lax.rsqrt(mean + epsilon) * hgain[...] * output_scale
    attbuf[core * ny + y] = attended.astype(BF16)
    mine = attbuf.at[core * ny + y]
    for k in far_first(ny):
        send(mine, mine, 7, {"kv_1": y_at(k)})
        send(mine, mine, 7, {"kv_1": y_at(k), "tp": other})
    send(mine, mine, 7, {"tp": other})

    all_of(kvbuf.at[pl.ds(0, ny - 1)], 3).wait_recv()
    for s in range(ny):
        out_ref[pl.ds(s, 1), pl.ds(128, 128)] = kvbuf[s, pl.ds(0, 1), :]
        out_ref[pl.ds(s, 1), pl.ds(256, 128)] = kvbuf[s, pl.ds(1, 1), :]
    all_of(outw.at[0], 8).wait_recv()

    all_of(attbuf.at[pl.ds(0, 2 * ny - 1)], 7).wait_recv()
    mixed = jnp.zeros((ny, 128), F32)
    for group in range(2):
        rows = jnp.concatenate(
            [attbuf[group * ny + s].astype(F32) for s in range(ny)], axis=0
        ).astype(BF16)
        product = lax.dot_general(
            rows, outw[group], (((1,), (1,)), ((), ())), preferred_element_type=F32
        )
        out_row = lax.broadcasted_iota(jnp.int32, product.shape, 0)
        out_lane = lax.broadcasted_iota(jnp.int32, product.shape, 1)
        product = jnp.where(lax.rem(out_row, heads) == out_lane // columns, product, 0.0)
        summed = jnp.sum(product.reshape(ny, heads, 128), axis=1)
        step = columns
        while step < 128:
            summed = summed + pltpu.roll(summed, step, 1)
            step *= 2
        mixed = mixed + summed.astype(BF16).astype(F32)
    out_ref[:, pl.ds(0, 128)] = mixed

    for which, ref in (
        (0, yrecv),
        (1, zbuf),
        (2, qbuf.at[pl.ds(0, len(near))]),
        (3, kvbuf.at[pl.ds(0, ny - 1)]),
        (4, brecv),
        (5, zw),
        (6, zst),
        (7, attbuf.at[pl.ds(0, 2 * ny - 1)]),
        (8, outw.at[0]),
        (9, kfar),
        (10, vfar),
    ):
        all_of(ref, which).wait_send()


def cut(x_ref, mixed_ref, nk_ref, nv_ref):
    mixed_ref[...] = x_ref[:, : mixed_ref.shape[1]].astype(BF16)
    nk_ref[...] = x_ref[:, 128:256].astype(BF16)
    nv_ref[...] = x_ref[:, 256:].astype(BF16)


def body(
    nz,
    ny,
    tokens,
    lengths,
    query_weight,
    key_weight,
    value_weight,
    query_gain,
    key_gain,
    lambdas,
    head_gain,
    out_weight,
    cache_keys,
    cache_values,
):
    sequences, positions = cache_keys.shape[:2]
    depth, width_q = query_weight.shape
    heads = width_q // 128
    rows2 = 2 * heads
    columns = out_weight.shape[1]
    half = query_gain.shape[0] // 2
    frequency = rotary_base ** (-np.arange(half, dtype=np.float64) / half)
    freq = jnp.asarray(np.tile(frequency, 4).astype(np.float32)[None, :])
    blocks = heads + 2
    any_space = pl.BlockSpec(memory_space=pl.ANY)
    vmem = pl.BlockSpec(memory_space=pltpu.VMEM)
    out = pl.pallas_call(
        functools.partial(kernel, nz, ny),
        name="decode_step",
        out_shape=pltpu.VMEM((sequences, 384), F32),
        in_specs=[any_space] * 13,
        out_specs=vmem,
        scratch_shapes=[
            pltpu.VMEM((sequences, depth), BF16),
            pltpu.VMEM((depth, width_q + 256), BF16),
            pltpu.SMEM((sequences,), jnp.int32),
            pltpu.VMEM((2, 1, 64), F32),
            pltpu.SMEM((heads,), F32),
            pltpu.VMEM((1, 128), F32),
            pltpu.VMEM((1, 128), F32),
            pltpu.VMEM((2, heads * columns, 128), BF16),
            pltpu.VMEM((sequences, positions, 128), BF16),
            pltpu.VMEM((sequences, positions, 128), BF16),
            pltpu.VMEM((sequences, blocks, 128), F32),
            pltpu.VMEM((ny, blocks, 128), F32),
            pltpu.VMEM((blocks, 128), F32),
            pltpu.VMEM((nz, blocks, 128), F32),
            pltpu.VMEM((ny, heads, 128), BF16),
            pltpu.VMEM((ny, 2, 128), F32),
            pltpu.VMEM((len(moved(ny)), positions, 128), BF16),
            pltpu.VMEM((len(moved(ny)), positions, 128), BF16),
            pltpu.VMEM((ny, rows2 + 2, 128), F32),
            pltpu.VMEM((len(near_first(ny)) + 1, rows2 + 2, 128), F32),
            pltpu.VMEM((rows2, 128), BF16),
            pltpu.VMEM((2, 128), F32),
            pltpu.VMEM((nz, rows2, 128), BF16),
            pltpu.VMEM((nz, 2, 128), F32),
            pltpu.VMEM((2 * ny, heads, 128), BF16),
            pltpu.SemaphoreType.DMA((12 + heads,)),
            pltpu.SemaphoreType.DMA((11,)),
            pltpu.SemaphoreType.DMA((11,)),
            pltpu.SemaphoreType.DMA((ny - 1,)),
            pltpu.SemaphoreType.REGULAR((4,)),
        ],
        compiler_params=pltpu.CompilerParams(collective_id=0, has_side_effects=True),
    )(
        tokens,
        lengths,
        query_weight,
        key_weight,
        value_weight,
        query_gain.reshape(1, -1),
        key_gain.reshape(1, -1),
        lambdas,
        head_gain.reshape(1, -1),
        out_weight.T,
        cache_keys.reshape(sequences, positions, 128),
        cache_values.reshape(sequences, positions, 128),
        freq,
    )
    mixed, new_keys, new_values = pl.pallas_call(
        cut,
        name="cut",
        out_shape=(
            jax.ShapeDtypeStruct((sequences, columns), BF16),
            jax.ShapeDtypeStruct((sequences, 128), BF16),
            jax.ShapeDtypeStruct((sequences, 128), BF16),
        ),
        in_specs=[vmem],
        out_specs=(vmem, vmem, vmem),
    )(pltpu.with_memory_space_constraint(out, pltpu.VMEM))
    return (
        mixed,
        new_keys.reshape(sequences, 1, 128),
        new_values.reshape(sequences, 1, 128),
    )


def solution(mesh):
    ny = 8
    nz = mesh.shape["kv"] // ny
    finer = Mesh(
        mesh.devices.reshape(mesh.shape["dp"], nz, ny, mesh.shape["tp"]),
        ("dp", "kv_0", "kv_1", "tp"),
    )
    in_specs = (
        P("dp", KV),
        P("dp"),
        P(KV, "tp"),
        P(KV, "tp"),
        P(KV, "tp"),
        P(),
        P(),
        P("tp"),
        P(),
        P("tp", KV),
        P("dp", KV, "tp", None),
        P("dp", KV, "tp", None),
    )
    out_specs = (P("dp", KV), P("dp", "tp", None), P("dp", "tp", None))
    return jax.shard_map(
        functools.partial(body, nz, ny),
        mesh=finer,
        in_specs=in_specs,
        out_specs=out_specs,
        check_vma=False,
    )
```

```python
import functools
import math

import jax
import jax.numpy as jnp
import numpy as np
from jax import lax
from jax.experimental import pallas as pl
from jax.experimental.pallas import tpu as pltpu
from jax.sharding import Mesh
from jax.sharding import PartitionSpec as P

KV = ("kv_0", "kv_1")
MESH = pl.DeviceIdType.MESH

epsilon = 1e-06
rotary_base = 10000.0
masked_score = -1e30
output_scale = 0.2 + 0.6 * math.exp(-0.3)
F32 = jnp.float32
BF16 = jnp.bfloat16


def far_first(n):
    return sorted(range(1, n), key=lambda k: -min(k, n - k))


def kernel(
    nz,
    ny,
    tok_hbm,
    len_hbm,
    wq_hbm,
    wk_hbm,
    wv_hbm,
    qg_hbm,
    kg_hbm,
    lam_hbm,
    hg_hbm,
    ow_hbm,
    ck_hbm,
    cv_hbm,
    freq_hbm,
    out_ref,
    tok,
    wts,
    lens,
    gains,
    lams,
    hgain,
    freq,
    outw,
    ck,
    cv,
    pbuf,
    yrecv,
    zsend,
    zbuf,
    qbuf,
    kvbuf,
    kside,
    vside,
    bmsg,
    brecv,
    zwsend,
    zstsend,
    zw,
    zst,
    attbuf,
    load_sem,
    send_sem,
    recv_sem,
    q_sem,
    gate_sem,
):
    y = lax.axis_index("kv_1")
    z = lax.axis_index("kv_0")
    core = lax.axis_index("tp")
    other = 1 - core
    positions = ck.shape[1]

    def y_at(k):
        return lax.rem(y + k, ny)

    def z_at(k):
        return lax.rem(z + k, nz)

    barrier = pltpu.get_barrier_semaphore()
    for k in far_first(ny):
        pl.semaphore_signal(barrier, 1, device_id={"kv_1": y_at(k), "tp": 1}, device_id_type=MESH)
    pl.semaphore_signal(barrier, 1, device_id={"tp": other}, device_id_type=MESH)
    for k in far_first(nz):
        pl.semaphore_signal(barrier, 1, device_id={"kv_0": z_at(k), "tp": 0}, device_id_type=MESH)

    width_q = wq_hbm.shape[1]
    loads = [
        pltpu.make_async_copy(tok_hbm, tok, load_sem.at[0]),
        pltpu.make_async_copy(wq_hbm, wts.at[:, pl.ds(0, width_q)], load_sem.at[1]),
        pltpu.make_async_copy(wk_hbm, wts.at[:, pl.ds(width_q, 128)], load_sem.at[2]),
        pltpu.make_async_copy(wv_hbm, wts.at[:, pl.ds(width_q + 128, 128)], load_sem.at[3]),
        pltpu.make_async_copy(len_hbm, lens, load_sem.at[4]),
        pltpu.make_async_copy(qg_hbm, gains.at[0], load_sem.at[5]),
        pltpu.make_async_copy(kg_hbm, gains.at[1], load_sem.at[6]),
        pltpu.make_async_copy(lam_hbm, lams, load_sem.at[7]),
        pltpu.make_async_copy(hg_hbm, hgain, load_sem.at[8]),
        pltpu.make_async_copy(freq_hbm, freq, load_sem.at[9]),
        pltpu.make_async_copy(ck_hbm, ck, load_sem.at[10]),
        pltpu.make_async_copy(cv_hbm, cv, load_sem.at[11]),
    ]
    heads = width_q // 128
    columns = ow_hbm.shape[0]
    for h in range(heads):
        loads.append(
            pltpu.make_async_copy(
                ow_hbm.at[:, pl.ds(128 * h, 128)],
                outw.at[core, pl.ds(columns * h, columns)],
                load_sem.at[12 + h],
            )
        )
    for load in loads:
        load.start()

    def tell_other(gate):
        pl.semaphore_signal(gate_sem.at[gate], 1, device_id={"tp": other}, device_id_type=MESH)

    def send(src, dst, which, target, recv=None):
        copy = pltpu.make_async_remote_copy(
            src_ref=src,
            dst_ref=dst,
            send_sem=send_sem.at[which],
            recv_sem=recv_sem.at[which] if recv is None else recv,
            device_id=target,
            device_id_type=MESH,
        )
        copy.start()

    def all_of(ref, which):
        return pltpu.make_async_remote_copy(
            src_ref=ref,
            dst_ref=ref,
            send_sem=send_sem.at[which],
            recv_sem=recv_sem.at[which],
            device_id={"tp": other},
            device_id_type=MESH,
        )

    for load in loads[:4]:
        load.wait()
    partial = jnp.dot(tok[...], wts[...], preferred_element_type=F32)
    blocks = heads + 2
    for c in range(blocks):
        pbuf[:, c, :] = partial[:, 128 * c : 128 * (c + 1)]

    @pl.when(core == 1)
    def _():
        pl.semaphore_wait(barrier, 2 * (ny - 1) + 1)
        tell_other(0)

    @pl.when(core == 0)
    def _():
        pl.semaphore_wait(gate_sem.at[0], 1)

    for k in far_first(ny):
        send(pbuf.at[y_at(k)], yrecv.at[k], 0, {"kv_1": y_at(k), "tp": other})
    send(pbuf.at[y], yrecv.at[0], 0, {"tp": other})
    half = positions // 2
    for d in (3, 2, 1):
        for side, sign in ((0, 1), (1, ny - 1)):
            target = {"kv_1": y_at(d * sign)}
            s = y_at((d + 1) * sign)
            rows_in = pl.ds(side * half, half) if d == 3 else pl.ds(0, positions)
            rows_out = pl.ds((d - 1) * positions, half if d == 3 else positions)
            send(ck_hbm.at[s, rows_in], kside.at[side, rows_out], 9 + side, target)
            send(cv_hbm.at[s, rows_in], vside.at[side, rows_out], 11 + side, target)

    for load in loads[4:10]:
        load.wait()
    lane = lax.broadcasted_iota(jnp.int32, (blocks, 128), 1)
    row = lax.broadcasted_iota(jnp.int32, (blocks, 128), 0)
    gain_q = jnp.concatenate([gains[0], gains[0]], axis=1)
    gain_k = jnp.concatenate([gains[1], gains[1]], axis=1)
    gain = jnp.where(row < heads, gain_q, gain_k)
    angle = lens[y].astype(F32) * freq[...]
    cosine = jnp.cos(angle)
    sine = jnp.sin(angle)
    head_row = lax.broadcasted_iota(jnp.int32, (heads, 128), 0)
    lam = jnp.zeros((heads, 128), F32)
    for h in range(heads):
        lam = jnp.where(head_row == h, lams[h], lam)

    @pl.when(core == 0)
    def _():
        pl.semaphore_wait(barrier, 2 * (nz - 1) + 1)
        tell_other(1)

    @pl.when(core == 1)
    def _():
        pl.semaphore_wait(gate_sem.at[1], 1)

    for load in loads[12:]:
        load.wait()
    send(outw.at[core], outw.at[core], 8, {"tp": other})

    all_of(yrecv, 0).wait_recv()
    total = yrecv[0]
    for k in range(1, ny):
        total = total + yrecv[k]

    zsend[...] = total
    for k in far_first(nz):
        send(zsend, zbuf.at[z], 1, {"kv_0": z_at(k), "tp": other})
    send(zsend, zbuf.at[z], 1, {"tp": other})
    all_of(zbuf, 1).wait_recv()
    proj = zbuf[0]
    for k in range(1, nz):
        proj = proj + zbuf[k]

    low = lane < 64
    squares = proj * proj
    mean_low = jnp.sum(jnp.where(low, squares, 0.0), axis=1, keepdims=True) / 64
    mean_high = jnp.sum(jnp.where(low, 0.0, squares), axis=1, keepdims=True) / 64
    inverse = jnp.where(low, lax.rsqrt(mean_low + epsilon), lax.rsqrt(mean_high + epsilon))
    normed = proj * inverse * gain
    partner = jnp.where(
        lax.rem(lane, 64) < 32, -pltpu.roll(normed, 96, 1), pltpu.roll(normed, 32, 1)
    )
    rotated = normed * cosine + partner * sine
    qbuf[y] = rotated[:heads].astype(BF16)
    kvbuf[y] = jnp.concatenate([rotated[heads : heads + 1], proj[heads + 1 :]], axis=0)
    near = (1, ny - 1)
    for k in near:
        send(qbuf.at[y], qbuf.at[y], 2, {"kv_1": y_at(k)}, q_sem.at[k - 1])
    for k in far_first(ny):
        send(kvbuf.at[y], kvbuf.at[y], 3, {"kv_1": y_at(k)})

    scale = 64 ** (-0.5)
    rows2 = 2 * heads
    wide_lane = lax.broadcasted_iota(jnp.int32, (rows2, 128), 1)
    wide_row = lax.broadcasted_iota(jnp.int32, (rows2, 128), 0)
    eye = wide_lane == wide_row
    half_low = lax.broadcasted_iota(jnp.int32, (heads, 128), 1) < 64
    position = lax.broadcasted_iota(jnp.int32, (rows2, positions), 1)

    def positions_of(where):
        return position + (z * ny + where) * positions

    def positions_beside(side):
        parts = [positions_of(y)]
        for d in (1, 2, 3):
            parts.append(positions_of(y_at(d if side == 1 else ny - d)))
        parts[3] = parts[3][:, side * half : (side + 1) * half]
        return jnp.concatenate(parts, axis=1)

    def to_row(column):
        return jnp.sum(jnp.where(eye, column, 0.0), axis=0, keepdims=True)

    def to_column(values):
        return jnp.sum(jnp.where(eye, values, 0.0), axis=1, keepdims=True)

    def two_maps(query):
        return jnp.concatenate(
            [jnp.where(half_low, query, 0.0), jnp.where(half_low, 0.0, query)], axis=0
        )

    def attend(s, blocks, where):
        query = two_maps(qbuf[s].astype(F32)).astype(BF16)
        scores = [
            lax.dot_general(query, keys, (((1,), (1,)), ((), ())), preferred_element_type=F32)
            for keys, _ in blocks
        ]
        scores = jnp.concatenate(scores, axis=1) * scale
        valid = where < lens[s]
        highest = jnp.max(jnp.where(valid, scores, masked_score), axis=1, keepdims=True)
        expo = jnp.where(valid, jnp.exp(scores - highest), 0.0)
        count = jnp.sum(expo, axis=1, keepdims=True)
        expo = expo.astype(BF16)
        at = 0
        weighted = jnp.zeros((rows2, 128), F32)
        for _, values in blocks:
            part = expo[:, at : at + values.shape[0]]
            weighted = weighted + jnp.dot(part, values, preferred_element_type=F32)
            at += values.shape[0]
        bmsg[s, pl.ds(0, rows2), :] = weighted
        bmsg[s, pl.ds(rows2, 2), :] = jnp.concatenate([to_row(highest), to_row(count)], axis=0)

    for load in loads[10:12]:
        load.wait()
    attend(y, [(ck[y], cv[y])], positions_of(y))
    send(bmsg.at[y], brecv.at[2], 4, {"tp": other})
    for side, k in ((1, 1), (0, ny - 1)):
        s = lax.rem(y + ny - k, ny)
        pltpu.make_async_remote_copy(
            src_ref=qbuf.at[s],
            dst_ref=qbuf.at[s],
            send_sem=send_sem.at[2],
            recv_sem=q_sem.at[k - 1],
            device_id={"kv_1": s},
            device_id_type=MESH,
        ).wait_recv()
        all_of(kside.at[side], 9 + side).wait_recv()
        all_of(vside.at[side], 11 + side).wait_recv()
        blocks = [(ck[s], cv[s]), (kside[side], vside[side])]
        attend(s, blocks, positions_beside(side))
        send(bmsg.at[s], brecv.at[side], 4, {"kv_1": s, "tp": other})

    own_query = two_maps(qbuf[y].astype(F32))
    own_key = kvbuf[y, pl.ds(0, 1), :].astype(BF16).astype(F32)
    own_value = kvbuf[y, pl.ds(1, 1), :].astype(BF16).astype(F32)
    own_score = to_row(jnp.sum(own_query * own_key, axis=1, keepdims=True) * scale)

    all_of(brecv, 4).wait_recv()
    parts = [brecv[i] for i in range(len(near) + 1)]
    highs = [part[rows2 : rows2 + 1] for part in parts]
    high = functools.reduce(jnp.maximum, highs)
    count = jnp.zeros_like(high)
    weighted = jnp.zeros((rows2, 128), F32)
    for part, one in zip(parts, highs):
        factor = jnp.exp(one - high)
        count = count + factor * part[rows2 + 1 :]
        weighted = weighted + to_column(factor) * part[:rows2]
    zwsend[...] = weighted.astype(BF16)
    zstsend[...] = jnp.concatenate([high, count], axis=0)
    for k in far_first(nz):
        send(zstsend, zst.at[z], 6, {"kv_0": z_at(k), "tp": other})
        send(zwsend, zw.at[z], 5, {"kv_0": z_at(k), "tp": other})
    send(zstsend, zst.at[z], 6, {"tp": other})
    send(zwsend, zw.at[z], 5, {"tp": other})
    all_of(zst, 6).wait_recv()
    stats = [zst[k] for k in range(nz)]
    high = own_score
    for stat in stats:
        high = jnp.maximum(high, stat[:1])
    own_weight = jnp.exp(own_score - high)
    count = own_weight
    factors = []
    for stat in stats:
        factor = jnp.exp(stat[:1] - high)
        factors.append(factor)
        count = count + factor * stat[1:]
    share = 1.0 / count
    attention = to_column(own_weight * share) * own_value
    columns_of = [to_column(factor * share) for factor in factors]
    all_of(zw, 5).wait_recv()
    for k in range(nz):
        attention = attention + columns_of[k] * zw[k].astype(F32)
    gaps = attention[:heads] - lam * attention[heads:]
    mean = jnp.sum(gaps * gaps, axis=1, keepdims=True) / 128
    attended = gaps * lax.rsqrt(mean + epsilon) * hgain[...] * output_scale
    attbuf[core * ny + y] = attended.astype(BF16)
    mine = attbuf.at[core * ny + y]
    for k in far_first(ny):
        send(mine, mine, 7, {"kv_1": y_at(k)})
        send(mine, mine, 7, {"kv_1": y_at(k), "tp": other})
    send(mine, mine, 7, {"tp": other})

    all_of(kvbuf.at[pl.ds(0, ny - 1)], 3).wait_recv()
    for s in range(ny):
        out_ref[pl.ds(s, 1), pl.ds(128, 128)] = kvbuf[s, pl.ds(0, 1), :]
        out_ref[pl.ds(s, 1), pl.ds(256, 128)] = kvbuf[s, pl.ds(1, 1), :]
    all_of(outw.at[0], 8).wait_recv()

    all_of(attbuf.at[pl.ds(0, 2 * ny - 1)], 7).wait_recv()
    mixed = jnp.zeros((ny, 128), F32)
    for group in range(2):
        rows = jnp.concatenate(
            [attbuf[group * ny + s].astype(F32) for s in range(ny)], axis=0
        ).astype(BF16)
        product = lax.dot_general(
            rows, outw[group], (((1,), (1,)), ((), ())), preferred_element_type=F32
        )
        out_row = lax.broadcasted_iota(jnp.int32, product.shape, 0)
        out_lane = lax.broadcasted_iota(jnp.int32, product.shape, 1)
        product = jnp.where(lax.rem(out_row, heads) == out_lane // columns, product, 0.0)
        summed = jnp.sum(product.reshape(ny, heads, 128), axis=1)
        step = columns
        while step < 128:
            summed = summed + pltpu.roll(summed, step, 1)
            step *= 2
        mixed = mixed + summed.astype(BF16).astype(F32)
    out_ref[:, pl.ds(0, 128)] = mixed

    for which, ref in (
        (0, yrecv),
        (1, zbuf),
        (2, qbuf.at[pl.ds(0, len(near))]),
        (3, kvbuf.at[pl.ds(0, ny - 1)]),
        (4, brecv),
        (5, zw),
        (6, zst),
        (7, attbuf.at[pl.ds(0, 2 * ny - 1)]),
        (8, outw.at[0]),
        (9, kside.at[0]),
        (10, kside.at[1]),
        (11, vside.at[0]),
        (12, vside.at[1]),
    ):
        all_of(ref, which).wait_send()


def cut(x_ref, mixed_ref, nk_ref, nv_ref):
    mixed_ref[...] = x_ref[:, : mixed_ref.shape[1]].astype(BF16)
    nk_ref[...] = x_ref[:, 128:256].astype(BF16)
    nv_ref[...] = x_ref[:, 256:].astype(BF16)


def body(
    nz,
    ny,
    tokens,
    lengths,
    query_weight,
    key_weight,
    value_weight,
    query_gain,
    key_gain,
    lambdas,
    head_gain,
    out_weight,
    cache_keys,
    cache_values,
):
    sequences, positions = cache_keys.shape[:2]
    depth, width_q = query_weight.shape
    heads = width_q // 128
    rows2 = 2 * heads
    columns = out_weight.shape[1]
    half = query_gain.shape[0] // 2
    frequency = rotary_base ** (-np.arange(half, dtype=np.float64) / half)
    freq = jnp.asarray(np.tile(frequency, 4).astype(np.float32)[None, :])
    blocks = heads + 2
    any_space = pl.BlockSpec(memory_space=pl.ANY)
    vmem = pl.BlockSpec(memory_space=pltpu.VMEM)
    out = pl.pallas_call(
        functools.partial(kernel, nz, ny),
        name="decode_step",
        out_shape=pltpu.VMEM((sequences, 384), F32),
        in_specs=[any_space] * 13,
        out_specs=vmem,
        scratch_shapes=[
            pltpu.VMEM((sequences, depth), BF16),
            pltpu.VMEM((depth, width_q + 256), BF16),
            pltpu.SMEM((sequences,), jnp.int32),
            pltpu.VMEM((2, 1, 64), F32),
            pltpu.SMEM((heads,), F32),
            pltpu.VMEM((1, 128), F32),
            pltpu.VMEM((1, 128), F32),
            pltpu.VMEM((2, heads * columns, 128), BF16),
            pltpu.VMEM((sequences, positions, 128), BF16),
            pltpu.VMEM((sequences, positions, 128), BF16),
            pltpu.VMEM((sequences, blocks, 128), F32),
            pltpu.VMEM((ny, blocks, 128), F32),
            pltpu.VMEM((blocks, 128), F32),
            pltpu.VMEM((nz, blocks, 128), F32),
            pltpu.VMEM((ny, heads, 128), BF16),
            pltpu.VMEM((ny, 2, 128), F32),
            pltpu.VMEM((2, 5 * positions // 2, 128), BF16),
            pltpu.VMEM((2, 5 * positions // 2, 128), BF16),
            pltpu.VMEM((ny, rows2 + 2, 128), F32),
            pltpu.VMEM((3, rows2 + 2, 128), F32),
            pltpu.VMEM((rows2, 128), BF16),
            pltpu.VMEM((2, 128), F32),
            pltpu.VMEM((nz, rows2, 128), BF16),
            pltpu.VMEM((nz, 2, 128), F32),
            pltpu.VMEM((2 * ny, heads, 128), BF16),
            pltpu.SemaphoreType.DMA((12 + heads,)),
            pltpu.SemaphoreType.DMA((13,)),
            pltpu.SemaphoreType.DMA((13,)),
            pltpu.SemaphoreType.DMA((ny - 1,)),
            pltpu.SemaphoreType.REGULAR((2,)),
        ],
        compiler_params=pltpu.CompilerParams(collective_id=0, has_side_effects=True),
    )(
        tokens,
        lengths,
        query_weight,
        key_weight,
        value_weight,
        query_gain.reshape(1, -1),
        key_gain.reshape(1, -1),
        lambdas,
        head_gain.reshape(1, -1),
        out_weight.T,
        cache_keys.reshape(sequences, positions, 128),
        cache_values.reshape(sequences, positions, 128),
        freq,
    )
    mixed, new_keys, new_values = pl.pallas_call(
        cut,
        name="cut",
        out_shape=(
            jax.ShapeDtypeStruct((sequences, columns), BF16),
            jax.ShapeDtypeStruct((sequences, 128), BF16),
            jax.ShapeDtypeStruct((sequences, 128), BF16),
        ),
        in_specs=[vmem],
        out_specs=(vmem, vmem, vmem),
    )(pltpu.with_memory_space_constraint(out, pltpu.VMEM))
    return (
        mixed,
        new_keys.reshape(sequences, 1, 128),
        new_values.reshape(sequences, 1, 128),
    )


def solution(mesh):
    ny = 8
    nz = mesh.shape["kv"] // ny
    finer = Mesh(
        mesh.devices.reshape(mesh.shape["dp"], nz, ny, mesh.shape["tp"]),
        ("dp", "kv_0", "kv_1", "tp"),
    )
    in_specs = (
        P("dp", KV),
        P("dp"),
        P(KV, "tp"),
        P(KV, "tp"),
        P(KV, "tp"),
        P(),
        P(),
        P("tp"),
        P(),
        P("tp", KV),
        P("dp", KV, "tp", None),
        P("dp", KV, "tp", None),
    )
    out_specs = (P("dp", KV), P("dp", "tp", None), P("dp", "tp", None))
    return jax.shard_map(
        functools.partial(body, nz, ny),
        mesh=finer,
        in_specs=in_specs,
        out_specs=out_specs,
        check_vma=False,
    )
```

```python
import functools
import math

import jax
import jax.numpy as jnp
import numpy as np
from jax import lax
from jax.experimental import pallas as pl
from jax.experimental.pallas import tpu as pltpu
from jax.sharding import Mesh
from jax.sharding import PartitionSpec as P

KV = ("kv_0", "kv_1")
MESH = pl.DeviceIdType.MESH

epsilon = 1e-06
rotary_base = 10000.0
masked_score = -1e30
output_scale = 0.2 + 0.6 * math.exp(-0.3)
F32 = jnp.float32
BF16 = jnp.bfloat16


def far_first(n):
    return sorted(range(1, n), key=lambda k: -min(k, n - k))


def kernel(
    nz,
    ny,
    tok_hbm,
    len_hbm,
    wq_hbm,
    wk_hbm,
    wv_hbm,
    qg_hbm,
    kg_hbm,
    lam_hbm,
    hg_hbm,
    ow_hbm,
    ck_hbm,
    cv_hbm,
    freq_hbm,
    out_ref,
    tok,
    wts,
    lens,
    gains,
    lams,
    hgain,
    freq,
    outw,
    ck,
    cv,
    pbuf,
    yrecv,
    zsend,
    zbuf,
    qbuf,
    kvbuf,
    kside,
    vside,
    bmsg,
    brecv,
    zwsend,
    zstsend,
    zw,
    zst,
    attbuf,
    load_sem,
    send_sem,
    recv_sem,
    q_sem,
    gate_sem,
):
    y = lax.axis_index("kv_1")
    z = lax.axis_index("kv_0")
    core = lax.axis_index("tp")
    other = 1 - core
    late = nz * 5 // 8
    positions = ck.shape[1]

    def y_at(k):
        return lax.rem(y + k, ny)

    def z_at(k):
        return lax.rem(z + k, nz)

    barrier = pltpu.get_barrier_semaphore()
    for k in far_first(ny):
        pl.semaphore_signal(barrier, 1, device_id={"kv_1": y_at(k), "tp": 1}, device_id_type=MESH)
    pl.semaphore_signal(barrier, 1, device_id={"tp": other}, device_id_type=MESH)
    for k in far_first(nz):
        pl.semaphore_signal(barrier, 1, device_id={"kv_0": z_at(k), "tp": 0}, device_id_type=MESH)

    width_q = wq_hbm.shape[1]
    loads = [
        pltpu.make_async_copy(tok_hbm, tok, load_sem.at[0]),
        pltpu.make_async_copy(wq_hbm, wts.at[:, pl.ds(0, width_q)], load_sem.at[1]),
        pltpu.make_async_copy(wk_hbm, wts.at[:, pl.ds(width_q, 128)], load_sem.at[2]),
        pltpu.make_async_copy(wv_hbm, wts.at[:, pl.ds(width_q + 128, 128)], load_sem.at[3]),
        pltpu.make_async_copy(len_hbm, lens, load_sem.at[4]),
        pltpu.make_async_copy(qg_hbm, gains.at[0], load_sem.at[5]),
        pltpu.make_async_copy(kg_hbm, gains.at[1], load_sem.at[6]),
        pltpu.make_async_copy(lam_hbm, lams, load_sem.at[7]),
        pltpu.make_async_copy(hg_hbm, hgain, load_sem.at[8]),
        pltpu.make_async_copy(freq_hbm, freq, load_sem.at[9]),
        pltpu.make_async_copy(ck_hbm, ck, load_sem.at[10]),
        pltpu.make_async_copy(cv_hbm, cv, load_sem.at[11]),
    ]
    heads = width_q // 128
    columns = ow_hbm.shape[0]
    for h in range(heads):
        loads.append(
            pltpu.make_async_copy(
                ow_hbm.at[:, pl.ds(128 * h, 128)],
                outw.at[core, pl.ds(columns * h, columns)],
                load_sem.at[12 + h],
            )
        )
    for load in loads:
        load.start()

    def tell_other(gate):
        pl.semaphore_signal(gate_sem.at[gate], 1, device_id={"tp": other}, device_id_type=MESH)

    def send(src, dst, which, target, recv=None):
        copy = pltpu.make_async_remote_copy(
            src_ref=src,
            dst_ref=dst,
            send_sem=send_sem.at[which],
            recv_sem=recv_sem.at[which] if recv is None else recv,
            device_id=target,
            device_id_type=MESH,
        )
        copy.start()

    def all_of(ref, which):
        return pltpu.make_async_remote_copy(
            src_ref=ref,
            dst_ref=ref,
            send_sem=send_sem.at[which],
            recv_sem=recv_sem.at[which],
            device_id={"tp": other},
            device_id_type=MESH,
        )

    for load in loads[:4]:
        load.wait()
    partial = jnp.dot(tok[...], wts[...], preferred_element_type=F32)
    blocks = heads + 2
    for c in range(blocks):
        pbuf[:, c, :] = partial[:, 128 * c : 128 * (c + 1)]

    @pl.when(core == 1)
    def _():
        pl.semaphore_wait(barrier, 2 * (ny - 1) + 1)
        tell_other(0)

    @pl.when(core == 0)
    def _():
        pl.semaphore_wait(gate_sem.at[0], 1)

    for k in far_first(ny):
        send(pbuf.at[y_at(k)], yrecv.at[k], 0, {"kv_1": y_at(k), "tp": other})
    send(pbuf.at[y], yrecv.at[0], 0, {"tp": other})
    half = positions // 2
    sides = ((0, 1), (1, ny - 1))
    middle = ny // 2

    def rows_at(reach):
        return (middle - reach - 1) * positions + half

    def move(reach):
        for d in range(middle, reach, -1):
            hops = d - reach
            for side, sign in sides:
                target = {"kv_1": y_at(hops * sign)}
                s = y_at(d * sign)
                rows_in = pl.ds(side * half, half) if d == middle else pl.ds(0, positions)
                rows_out = pl.ds((hops - 1) * positions, half if d == middle else positions)
                send(ck_hbm.at[s, rows_in], kside.at[side, rows_out], 9 + side, target)
                send(cv_hbm.at[s, rows_in], vside.at[side, rows_out], 11 + side, target)

    def by_row(step):
        @pl.when(z < late)
        def _():
            step(1)

        @pl.when(z >= late)
        def _():
            step(2)

    by_row(move)

    for load in loads[4:10]:
        load.wait()
    lane = lax.broadcasted_iota(jnp.int32, (blocks, 128), 1)
    row = lax.broadcasted_iota(jnp.int32, (blocks, 128), 0)
    gain_q = jnp.concatenate([gains[0], gains[0]], axis=1)
    gain_k = jnp.concatenate([gains[1], gains[1]], axis=1)
    gain = jnp.where(row < heads, gain_q, gain_k)
    angle = lens[y].astype(F32) * freq[...]
    cosine = jnp.cos(angle)
    sine = jnp.sin(angle)
    head_row = lax.broadcasted_iota(jnp.int32, (heads, 128), 0)
    lam = jnp.zeros((heads, 128), F32)
    for h in range(heads):
        lam = jnp.where(head_row == h, lams[h], lam)

    @pl.when(core == 0)
    def _():
        pl.semaphore_wait(barrier, 2 * (nz - 1) + 1)
        tell_other(1)

    @pl.when(core == 1)
    def _():
        pl.semaphore_wait(gate_sem.at[1], 1)

    for load in loads[12:]:
        load.wait()
    send(outw.at[core], outw.at[core], 8, {"tp": other})

    all_of(yrecv, 0).wait_recv()
    total = yrecv[0]
    for k in range(1, ny):
        total = total + yrecv[k]

    zsend[...] = total
    for k in far_first(nz):
        send(zsend, zbuf.at[z], 1, {"kv_0": z_at(k), "tp": other})
    send(zsend, zbuf.at[z], 1, {"tp": other})
    all_of(zbuf, 1).wait_recv()
    proj = zbuf[0]
    for k in range(1, nz):
        proj = proj + zbuf[k]

    low = lane < 64
    squares = proj * proj
    mean_low = jnp.sum(jnp.where(low, squares, 0.0), axis=1, keepdims=True) / 64
    mean_high = jnp.sum(jnp.where(low, 0.0, squares), axis=1, keepdims=True) / 64
    inverse = jnp.where(low, lax.rsqrt(mean_low + epsilon), lax.rsqrt(mean_high + epsilon))
    normed = proj * inverse * gain
    partner = jnp.where(
        lax.rem(lane, 64) < 32, -pltpu.roll(normed, 96, 1), pltpu.roll(normed, 32, 1)
    )
    rotated = normed * cosine + partner * sine
    qbuf[y] = rotated[:heads].astype(BF16)
    kvbuf[y] = jnp.concatenate([rotated[heads : heads + 1], proj[heads + 1 :]], axis=0)

    def ask(reach):
        for e in range(reach, 0, -1):
            for _, sign in sides:
                k = e * sign % ny
                send(qbuf.at[y], qbuf.at[y], 2, {"kv_1": y_at(k)}, q_sem.at[k - 1])

    by_row(ask)
    for k in far_first(ny):
        send(kvbuf.at[y], kvbuf.at[y], 3, {"kv_1": y_at(k)})

    scale = 64 ** (-0.5)
    rows2 = 2 * heads
    wide_lane = lax.broadcasted_iota(jnp.int32, (rows2, 128), 1)
    wide_row = lax.broadcasted_iota(jnp.int32, (rows2, 128), 0)
    eye = wide_lane == wide_row
    half_low = lax.broadcasted_iota(jnp.int32, (heads, 128), 1) < 64
    position = lax.broadcasted_iota(jnp.int32, (rows2, positions), 1)

    def positions_of(where):
        return position + (z * ny + where) * positions

    def positions_beside(side, reach):
        parts = [positions_of(y)]
        for hops in range(1, middle - reach + 1):
            parts.append(positions_of(y_at(hops if side == 1 else ny - hops)))
        parts[-1] = parts[-1][:, side * half : (side + 1) * half]
        return jnp.concatenate(parts, axis=1)

    def to_row(column):
        return jnp.sum(jnp.where(eye, column, 0.0), axis=0, keepdims=True)

    def to_column(values):
        return jnp.sum(jnp.where(eye, values, 0.0), axis=1, keepdims=True)

    def two_maps(query):
        return jnp.concatenate(
            [jnp.where(half_low, query, 0.0), jnp.where(half_low, 0.0, query)], axis=0
        )

    def attend(s, blocks, where):
        query = two_maps(qbuf[s].astype(F32)).astype(BF16)
        scores = [
            lax.dot_general(query, keys, (((1,), (1,)), ((), ())), preferred_element_type=F32)
            for keys, _ in blocks
        ]
        scores = jnp.concatenate(scores, axis=1) * scale
        valid = where < lens[s]
        highest = jnp.max(jnp.where(valid, scores, masked_score), axis=1, keepdims=True)
        expo = jnp.where(valid, jnp.exp(scores - highest), 0.0)
        count = jnp.sum(expo, axis=1, keepdims=True)
        expo = expo.astype(BF16)
        at = 0
        weighted = jnp.zeros((rows2, 128), F32)
        for _, values in blocks:
            part = expo[:, at : at + values.shape[0]]
            weighted = weighted + jnp.dot(part, values, preferred_element_type=F32)
            at += values.shape[0]
        bmsg[s, pl.ds(0, rows2), :] = weighted
        bmsg[s, pl.ds(rows2, 2), :] = jnp.concatenate([to_row(highest), to_row(count)], axis=0)

    for load in loads[10:12]:
        load.wait()
    attend(y, [(ck[y], cv[y])], positions_of(y))
    send(bmsg.at[y], brecv.at[4], 4, {"tp": other})

    def answer(reach):
        for e in range(1, reach + 1):
            for side, sign in sides:
                k = e * sign % ny
                s = y_at(k)
                pltpu.make_async_remote_copy(
                    src_ref=qbuf.at[s],
                    dst_ref=qbuf.at[s],
                    send_sem=send_sem.at[2],
                    recv_sem=q_sem.at[ny - k - 1],
                    device_id={"kv_1": s},
                    device_id_type=MESH,
                ).wait_recv()
                blocks, where = [(ck[s], cv[s])], positions_of(y)
                if e == reach:
                    keys = kside.at[side, pl.ds(0, rows_at(reach))]
                    values = vside.at[side, pl.ds(0, rows_at(reach))]
                    all_of(keys, 9 + side).wait_recv()
                    all_of(values, 11 + side).wait_recv()
                    blocks.append((keys[...], values[...]))
                    where = positions_beside(side, reach)
                attend(s, blocks, where)
                send(bmsg.at[s], brecv.at[2 * (e - 1) + side], 4, {"kv_1": s, "tp": other})
        if reach == 1:
            nothing = jnp.full((1, 128), masked_score, F32)
            for slot in (2, 3):
                brecv[slot, pl.ds(0, rows2), :] = jnp.zeros((rows2, 128), F32)
                brecv[slot, pl.ds(rows2, 1), :] = nothing
                brecv[slot, pl.ds(rows2 + 1, 1), :] = jnp.zeros((1, 128), F32)

    by_row(answer)

    own_query = two_maps(qbuf[y].astype(F32))
    own_key = kvbuf[y, pl.ds(0, 1), :].astype(BF16).astype(F32)
    own_value = kvbuf[y, pl.ds(1, 1), :].astype(BF16).astype(F32)
    own_score = to_row(jnp.sum(own_query * own_key, axis=1, keepdims=True) * scale)

    by_row(lambda reach: all_of(brecv.at[pl.ds(0, 2 * reach + 1)], 4).wait_recv())
    parts = [brecv[i] for i in range(5)]
    highs = [part[rows2 : rows2 + 1] for part in parts]
    high = functools.reduce(jnp.maximum, highs)
    count = jnp.zeros_like(high)
    weighted = jnp.zeros((rows2, 128), F32)
    for part, one in zip(parts, highs):
        factor = jnp.exp(one - high)
        count = count + factor * part[rows2 + 1 :]
        weighted = weighted + to_column(factor) * part[:rows2]
    zwsend[...] = weighted.astype(BF16)
    zstsend[...] = jnp.concatenate([high, count], axis=0)
    for target in range(nz):
        send(zstsend, zst.at[z], 6, {"kv_0": target, "tp": other})
        send(zwsend, zw.at[z], 5, {"kv_0": target, "tp": other})
    all_of(zst, 6).wait_recv()
    stats = [zst[k] for k in range(nz)]
    high = own_score
    for stat in stats:
        high = jnp.maximum(high, stat[:1])
    own_weight = jnp.exp(own_score - high)
    count = own_weight
    factors = []
    for stat in stats:
        factor = jnp.exp(stat[:1] - high)
        factors.append(factor)
        count = count + factor * stat[1:]
    share = 1.0 / count
    attention = to_column(own_weight * share) * own_value
    columns_of = [to_column(factor * share) for factor in factors]
    all_of(zw, 5).wait_recv()
    for k in range(nz):
        attention = attention + columns_of[k] * zw[k].astype(F32)
    gaps = attention[:heads] - lam * attention[heads:]
    mean = jnp.sum(gaps * gaps, axis=1, keepdims=True) / 128
    attended = gaps * lax.rsqrt(mean + epsilon) * hgain[...] * output_scale
    attbuf[core * ny + y] = attended.astype(BF16)
    mine = attbuf.at[core * ny + y]
    for k in far_first(ny):
        send(mine, mine, 7, {"kv_1": y_at(k)})
        send(mine, mine, 7, {"kv_1": y_at(k), "tp": other})
    send(mine, mine, 7, {"tp": other})

    all_of(kvbuf.at[pl.ds(0, ny - 1)], 3).wait_recv()
    for s in range(ny):
        out_ref[pl.ds(s, 1), pl.ds(128, 128)] = kvbuf[s, pl.ds(0, 1), :]
        out_ref[pl.ds(s, 1), pl.ds(256, 128)] = kvbuf[s, pl.ds(1, 1), :]
    all_of(outw.at[0], 8).wait_recv()

    all_of(attbuf.at[pl.ds(0, 2 * ny - 1)], 7).wait_recv()
    mixed = jnp.zeros((ny, 128), F32)
    for group in range(2):
        rows = jnp.concatenate(
            [attbuf[group * ny + s].astype(F32) for s in range(ny)], axis=0
        ).astype(BF16)
        product = lax.dot_general(
            rows, outw[group], (((1,), (1,)), ((), ())), preferred_element_type=F32
        )
        out_row = lax.broadcasted_iota(jnp.int32, product.shape, 0)
        out_lane = lax.broadcasted_iota(jnp.int32, product.shape, 1)
        product = jnp.where(lax.rem(out_row, heads) == out_lane // columns, product, 0.0)
        summed = jnp.sum(product.reshape(ny, heads, 128), axis=1)
        step = columns
        while step < 128:
            summed = summed + pltpu.roll(summed, step, 1)
            step *= 2
        mixed = mixed + summed.astype(BF16).astype(F32)
    out_ref[:, pl.ds(0, 128)] = mixed

    for which, ref in (
        (0, yrecv),
        (1, zbuf),
        (3, kvbuf.at[pl.ds(0, ny - 1)]),
        (5, zw),
        (6, zst),
        (7, attbuf.at[pl.ds(0, 2 * ny - 1)]),
        (8, outw.at[0]),
    ):
        all_of(ref, which).wait_send()

    def drain(reach):
        all_of(qbuf.at[pl.ds(0, 2 * reach)], 2).wait_send()
        all_of(brecv.at[pl.ds(0, 2 * reach + 1)], 4).wait_send()
        for side in range(2):
            all_of(kside.at[side, pl.ds(0, rows_at(reach))], 9 + side).wait_send()
            all_of(vside.at[side, pl.ds(0, rows_at(reach))], 11 + side).wait_send()

    by_row(drain)


def cut(x_ref, mixed_ref, nk_ref, nv_ref):
    mixed_ref[...] = x_ref[:, : mixed_ref.shape[1]].astype(BF16)
    nk_ref[...] = x_ref[:, 128:256].astype(BF16)
    nv_ref[...] = x_ref[:, 256:].astype(BF16)


def body(
    nz,
    ny,
    tokens,
    lengths,
    query_weight,
    key_weight,
    value_weight,
    query_gain,
    key_gain,
    lambdas,
    head_gain,
    out_weight,
    cache_keys,
    cache_values,
):
    sequences, positions = cache_keys.shape[:2]
    depth, width_q = query_weight.shape
    heads = width_q // 128
    rows2 = 2 * heads
    columns = out_weight.shape[1]
    half = query_gain.shape[0] // 2
    frequency = rotary_base ** (-np.arange(half, dtype=np.float64) / half)
    freq = jnp.asarray(np.tile(frequency, 4).astype(np.float32)[None, :])
    blocks = heads + 2
    any_space = pl.BlockSpec(memory_space=pl.ANY)
    vmem = pl.BlockSpec(memory_space=pltpu.VMEM)
    out = pl.pallas_call(
        functools.partial(kernel, nz, ny),
        name="decode_step",
        out_shape=pltpu.VMEM((sequences, 384), F32),
        in_specs=[any_space] * 13,
        out_specs=vmem,
        scratch_shapes=[
            pltpu.VMEM((sequences, depth), BF16),
            pltpu.VMEM((depth, width_q + 256), BF16),
            pltpu.SMEM((sequences,), jnp.int32),
            pltpu.VMEM((2, 1, 64), F32),
            pltpu.SMEM((heads,), F32),
            pltpu.VMEM((1, 128), F32),
            pltpu.VMEM((1, 128), F32),
            pltpu.VMEM((2, heads * columns, 128), BF16),
            pltpu.VMEM((sequences, positions, 128), BF16),
            pltpu.VMEM((sequences, positions, 128), BF16),
            pltpu.VMEM((sequences, blocks, 128), F32),
            pltpu.VMEM((ny, blocks, 128), F32),
            pltpu.VMEM((blocks, 128), F32),
            pltpu.VMEM((nz, blocks, 128), F32),
            pltpu.VMEM((ny, heads, 128), BF16),
            pltpu.VMEM((ny, 2, 128), F32),
            pltpu.VMEM((2, 5 * positions // 2, 128), BF16),
            pltpu.VMEM((2, 5 * positions // 2, 128), BF16),
            pltpu.VMEM((ny, rows2 + 2, 128), F32),
            pltpu.VMEM((5, rows2 + 2, 128), F32),
            pltpu.VMEM((rows2, 128), BF16),
            pltpu.VMEM((2, 128), F32),
            pltpu.VMEM((nz, rows2, 128), BF16),
            pltpu.VMEM((nz, 2, 128), F32),
            pltpu.VMEM((2 * ny, heads, 128), BF16),
            pltpu.SemaphoreType.DMA((12 + heads,)),
            pltpu.SemaphoreType.DMA((13,)),
            pltpu.SemaphoreType.DMA((13,)),
            pltpu.SemaphoreType.DMA((ny - 1,)),
            pltpu.SemaphoreType.REGULAR((2,)),
        ],
        compiler_params=pltpu.CompilerParams(collective_id=0, has_side_effects=True),
    )(
        tokens,
        lengths,
        query_weight,
        key_weight,
        value_weight,
        query_gain.reshape(1, -1),
        key_gain.reshape(1, -1),
        lambdas,
        head_gain.reshape(1, -1),
        out_weight.T,
        cache_keys.reshape(sequences, positions, 128),
        cache_values.reshape(sequences, positions, 128),
        freq,
    )
    mixed, new_keys, new_values = pl.pallas_call(
        cut,
        name="cut",
        out_shape=(
            jax.ShapeDtypeStruct((sequences, columns), BF16),
            jax.ShapeDtypeStruct((sequences, 128), BF16),
            jax.ShapeDtypeStruct((sequences, 128), BF16),
        ),
        in_specs=[vmem],
        out_specs=(vmem, vmem, vmem),
    )(pltpu.with_memory_space_constraint(out, pltpu.VMEM))
    return (
        mixed,
        new_keys.reshape(sequences, 1, 128),
        new_values.reshape(sequences, 1, 128),
    )


def solution(mesh):
    ny = 8
    nz = mesh.shape["kv"] // ny
    finer = Mesh(
        mesh.devices.reshape(mesh.shape["dp"], nz, ny, mesh.shape["tp"]),
        ("dp", "kv_0", "kv_1", "tp"),
    )
    in_specs = (
        P("dp", KV),
        P("dp"),
        P(KV, "tp"),
        P(KV, "tp"),
        P(KV, "tp"),
        P(),
        P(),
        P("tp"),
        P(),
        P("tp", KV),
        P("dp", KV, "tp", None),
        P("dp", KV, "tp", None),
    )
    out_specs = (P("dp", KV), P("dp", "tp", None), P("dp", "tp", None))
    return jax.shard_map(
        functools.partial(body, nz, ny),
        mesh=finer,
        in_specs=in_specs,
        out_specs=out_specs,
        check_vma=False,
    )
```

```python
import functools
import math

import jax
import jax.numpy as jnp
import numpy as np
from jax import lax
from jax.experimental import pallas as pl
from jax.experimental.pallas import tpu as pltpu
from jax.sharding import Mesh
from jax.sharding import PartitionSpec as P

KV = ("kv_0", "kv_1")
MESH = pl.DeviceIdType.MESH

epsilon = 1e-06
rotary_base = 10000.0
masked_score = -1e30
output_scale = 0.2 + 0.6 * math.exp(-0.3)
F32 = jnp.float32
BF16 = jnp.bfloat16


def far_first(n):
    return sorted(range(1, n), key=lambda k: -min(k, n - k))


def kernel(
    nz,
    ny,
    tok_hbm,
    len_hbm,
    wq_hbm,
    wk_hbm,
    wv_hbm,
    qg_hbm,
    kg_hbm,
    lam_hbm,
    hg_hbm,
    ow_hbm,
    ck_hbm,
    cv_hbm,
    freq_hbm,
    out_ref,
    tok,
    wts,
    lens,
    gains,
    lams,
    hgain,
    freq,
    outw,
    ck,
    cv,
    pbuf,
    yrecv,
    zsend,
    zbuf,
    qother,
    kvother,
    qbuf,
    kvbuf,
    kside,
    vside,
    bmsg,
    brecv,
    zwsend,
    zstsend,
    zw,
    zst,
    attbuf,
    load_sem,
    send_sem,
    recv_sem,
    q_sem,
    gate_sem,
):
    y = lax.axis_index("kv_1")
    z = lax.axis_index("kv_0")
    core = lax.axis_index("tp")
    other = 1 - core
    late = nz * 5 // 8
    positions = ck.shape[1]

    def y_at(k):
        return lax.rem(y + k, ny)

    def z_at(k):
        return lax.rem(z + k, nz)

    barrier = pltpu.get_barrier_semaphore()
    for k in far_first(ny):
        pl.semaphore_signal(barrier, 1, device_id={"kv_1": y_at(k), "tp": 1}, device_id_type=MESH)
    pl.semaphore_signal(barrier, 1, device_id={"tp": other}, device_id_type=MESH)
    for k in far_first(nz):
        pl.semaphore_signal(barrier, 1, device_id={"kv_0": z_at(k), "tp": 0}, device_id_type=MESH)

    width_q = wq_hbm.shape[1]
    loads = [
        pltpu.make_async_copy(tok_hbm, tok, load_sem.at[0]),
        pltpu.make_async_copy(wq_hbm, wts.at[:, pl.ds(0, width_q)], load_sem.at[1]),
        pltpu.make_async_copy(wk_hbm, wts.at[:, pl.ds(width_q, 128)], load_sem.at[2]),
        pltpu.make_async_copy(wv_hbm, wts.at[:, pl.ds(width_q + 128, 128)], load_sem.at[3]),
        pltpu.make_async_copy(len_hbm, lens, load_sem.at[4]),
        pltpu.make_async_copy(qg_hbm, gains.at[0], load_sem.at[5]),
        pltpu.make_async_copy(kg_hbm, gains.at[1], load_sem.at[6]),
        pltpu.make_async_copy(lam_hbm, lams, load_sem.at[7]),
        pltpu.make_async_copy(hg_hbm, hgain, load_sem.at[8]),
        pltpu.make_async_copy(freq_hbm, freq, load_sem.at[9]),
        pltpu.make_async_copy(ck_hbm, ck, load_sem.at[10]),
        pltpu.make_async_copy(cv_hbm, cv, load_sem.at[11]),
    ]
    heads = width_q // 128
    columns = ow_hbm.shape[0]
    for h in range(heads):
        loads.append(
            pltpu.make_async_copy(
                ow_hbm.at[:, pl.ds(128 * h, 128)],
                outw.at[core, pl.ds(columns * h, columns)],
                load_sem.at[12 + h],
            )
        )
    for load in loads:
        load.start()

    def tell_other(gate):
        pl.semaphore_signal(gate_sem.at[gate], 1, device_id={"tp": other}, device_id_type=MESH)

    def send(src, dst, which, target, recv=None):
        copy = pltpu.make_async_remote_copy(
            src_ref=src,
            dst_ref=dst,
            send_sem=send_sem.at[which],
            recv_sem=recv_sem.at[which] if recv is None else recv,
            device_id=target,
            device_id_type=MESH,
        )
        copy.start()

    def all_of(ref, which):
        return pltpu.make_async_remote_copy(
            src_ref=ref,
            dst_ref=ref,
            send_sem=send_sem.at[which],
            recv_sem=recv_sem.at[which],
            device_id={"tp": other},
            device_id_type=MESH,
        )

    for load in loads[:4]:
        load.wait()
    partial = jnp.dot(tok[...], wts[...], preferred_element_type=F32)
    blocks = heads + 2
    for c in range(blocks):
        pbuf[:, c, :] = partial[:, 128 * c : 128 * (c + 1)]

    @pl.when(core == 1)
    def _():
        pl.semaphore_wait(barrier, 2 * (ny - 1) + 1)
        tell_other(0)

    @pl.when(core == 0)
    def _():
        pl.semaphore_wait(gate_sem.at[0], 1)

    for k in far_first(ny):
        send(pbuf.at[y_at(k)], yrecv.at[k], 0, {"kv_1": y_at(k), "tp": other})
    send(pbuf.at[y], yrecv.at[0], 0, {"tp": other})
    half = positions // 2
    sides = ((0, 1), (1, ny - 1))
    middle = ny // 2

    def rows_at(reach):
        return (middle - reach - 1) * positions + half

    def move(reach):
        for d in range(middle, reach, -1):
            hops = d - reach
            for side, sign in sides:
                target = {"kv_1": y_at(hops * sign)}
                s = y_at(d * sign)
                rows_in = pl.ds(side * half, half) if d == middle else pl.ds(0, positions)
                rows_out = pl.ds((hops - 1) * positions, half if d == middle else positions)
                send(ck_hbm.at[s, rows_in], kside.at[side, rows_out], 9 + side, target)
                send(cv_hbm.at[s, rows_in], vside.at[side, rows_out], 11 + side, target)

    def by_row(step):
        @pl.when(z < late)
        def _():
            step(1)

        @pl.when(z >= late)
        def _():
            step(2)

    by_row(move)

    for load in loads[4:10]:
        load.wait()
    lane = lax.broadcasted_iota(jnp.int32, (blocks, 128), 1)
    row = lax.broadcasted_iota(jnp.int32, (blocks, 128), 0)
    gain_q = jnp.concatenate([gains[0], gains[0]], axis=1)
    gain_k = jnp.concatenate([gains[1], gains[1]], axis=1)
    gain = jnp.where(row < heads, gain_q, gain_k)
    angle = lens[y].astype(F32) * freq[...]
    cosine = jnp.cos(angle)
    sine = jnp.sin(angle)
    head_row = lax.broadcasted_iota(jnp.int32, (heads, 128), 0)
    lam = jnp.zeros((heads, 128), F32)
    for h in range(heads):
        lam = jnp.where(head_row == h, lams[h], lam)

    @pl.when(core == 0)
    def _():
        pl.semaphore_wait(barrier, 2 * (nz - 1) + 1)
        tell_other(1)

    @pl.when(core == 1)
    def _():
        pl.semaphore_wait(gate_sem.at[1], 1)

    for load in loads[12:]:
        load.wait()
    send(outw.at[core], outw.at[core], 8, {"tp": other})

    all_of(yrecv, 0).wait_recv()
    total = yrecv[0]
    for k in range(1, ny):
        total = total + yrecv[k]

    zsend[...] = total
    for k in far_first(nz):
        send(zsend, zbuf.at[other * nz + z], 1, {"kv_0": z_at(k), "tp": 1})

    @pl.when(core == 0)
    def _():
        send(zsend, zbuf.at[other * nz + z], 1, {"tp": 1})

    @pl.when(core == 1)
    def _():
        zbuf[z] = total
        all_of(zbuf.at[pl.ds(0, 2 * nz - 1)], 1).wait_recv()
        low = lane < 64
        for group in range(2):
            proj = zbuf[group * nz]
            for k in range(1, nz):
                proj = proj + zbuf[group * nz + k]
            squares = proj * proj
            mean_low = jnp.sum(jnp.where(low, squares, 0.0), axis=1, keepdims=True) / 64
            mean_high = jnp.sum(jnp.where(low, 0.0, squares), axis=1, keepdims=True) / 64
            inverse = jnp.where(
                low, lax.rsqrt(mean_low + epsilon), lax.rsqrt(mean_high + epsilon)
            )
            normed = proj * inverse * gain
            partner = jnp.where(
                lax.rem(lane, 64) < 32, -pltpu.roll(normed, 96, 1), pltpu.roll(normed, 32, 1)
            )
            rotated = normed * cosine + partner * sine
            query = rotated[:heads].astype(BF16)
            entry = jnp.concatenate(
                [rotated[heads : heads + 1], proj[heads + 1 :]], axis=0
            )
            if group == 0:
                qother[...] = query
                kvother[...] = entry
            else:
                qbuf[y] = query
                kvbuf[y] = entry

    def ask(reach):
        @pl.when(core == 1)
        def _():
            for e in range(reach, 0, -1):
                for _, sign in sides:
                    k = e * sign % ny
                    target = {"kv_1": y_at(k), "tp": 0}
                    send(qother, qbuf.at[y], 14, target, q_sem.at[k - 1])
            for e in range(reach, 0, -1):
                for _, sign in sides:
                    k = e * sign % ny
                    send(qbuf.at[y], qbuf.at[y], 2, {"kv_1": y_at(k)}, q_sem.at[k - 1])

    by_row(ask)

    @pl.when(core == 1)
    def _():
        send(qother, qbuf.at[y], 15, {"tp": 0}, q_sem.at[ny - 1])
        send(kvother, kvbuf.at[y], 13, {"tp": 0})
        for k in far_first(ny):
            target = {"kv_1": y_at(k), "tp": 0}
            send(kvother, kvbuf.at[y], 16, target, recv_sem.at[3])
            send(kvbuf.at[y], kvbuf.at[y], 3, {"kv_1": y_at(k)})

    scale = 64 ** (-0.5)
    rows2 = 2 * heads
    wide_lane = lax.broadcasted_iota(jnp.int32, (rows2, 128), 1)
    wide_row = lax.broadcasted_iota(jnp.int32, (rows2, 128), 0)
    eye = wide_lane == wide_row
    half_low = lax.broadcasted_iota(jnp.int32, (heads, 128), 1) < 64
    position = lax.broadcasted_iota(jnp.int32, (rows2, positions), 1)

    def positions_of(where):
        return position + (z * ny + where) * positions

    def positions_beside(side, reach):
        parts = [positions_of(y)]
        for hops in range(1, middle - reach + 1):
            parts.append(positions_of(y_at(hops if side == 1 else ny - hops)))
        parts[-1] = parts[-1][:, side * half : (side + 1) * half]
        return jnp.concatenate(parts, axis=1)

    def to_row(column):
        return jnp.sum(jnp.where(eye, column, 0.0), axis=0, keepdims=True)

    def to_column(values):
        return jnp.sum(jnp.where(eye, values, 0.0), axis=1, keepdims=True)

    def two_maps(query):
        return jnp.concatenate(
            [jnp.where(half_low, query, 0.0), jnp.where(half_low, 0.0, query)], axis=0
        )

    def attend(s, blocks, where):
        query = two_maps(qbuf[s].astype(F32)).astype(BF16)
        scores = [
            lax.dot_general(query, keys, (((1,), (1,)), ((), ())), preferred_element_type=F32)
            for keys, _ in blocks
        ]
        scores = jnp.concatenate(scores, axis=1) * scale
        valid = where < lens[s]
        highest = jnp.max(jnp.where(valid, scores, masked_score), axis=1, keepdims=True)
        expo = jnp.where(valid, jnp.exp(scores - highest), 0.0)
        count = jnp.sum(expo, axis=1, keepdims=True)
        expo = expo.astype(BF16)
        at = 0
        weighted = jnp.zeros((rows2, 128), F32)
        for _, values in blocks:
            part = expo[:, at : at + values.shape[0]]
            weighted = weighted + jnp.dot(part, values, preferred_element_type=F32)
            at += values.shape[0]
        bmsg[s, pl.ds(0, rows2), :] = weighted
        bmsg[s, pl.ds(rows2, 2), :] = jnp.concatenate([to_row(highest), to_row(count)], axis=0)

    for load in loads[10:12]:
        load.wait()
    @pl.when(core == 0)
    def _():
        pltpu.make_async_remote_copy(
            src_ref=qother,
            dst_ref=qbuf.at[y],
            send_sem=send_sem.at[15],
            recv_sem=q_sem.at[ny - 1],
            device_id={"tp": other},
            device_id_type=MESH,
        ).wait_recv()
        all_of(kvother, 13).wait_recv()

    attend(y, [(ck[y], cv[y])], positions_of(y))
    send(bmsg.at[y], brecv.at[4], 4, {"tp": other})

    def answer(reach):
        for e in range(1, reach + 1):
            for side, sign in sides:
                k = e * sign % ny
                s = y_at(k)
                pltpu.make_async_remote_copy(
                    src_ref=qbuf.at[s],
                    dst_ref=qbuf.at[s],
                    send_sem=send_sem.at[2],
                    recv_sem=q_sem.at[ny - k - 1],
                    device_id={"kv_1": s},
                    device_id_type=MESH,
                ).wait_recv()
                blocks, where = [(ck[s], cv[s])], positions_of(y)
                if e == reach:
                    keys = kside.at[side, pl.ds(0, rows_at(reach))]
                    values = vside.at[side, pl.ds(0, rows_at(reach))]
                    all_of(keys, 9 + side).wait_recv()
                    all_of(values, 11 + side).wait_recv()
                    blocks.append((keys[...], values[...]))
                    where = positions_beside(side, reach)
                attend(s, blocks, where)
                send(bmsg.at[s], brecv.at[2 * (e - 1) + side], 4, {"kv_1": s, "tp": other})
        if reach == 1:
            nothing = jnp.full((1, 128), masked_score, F32)
            for slot in (2, 3):
                brecv[slot, pl.ds(0, rows2), :] = jnp.zeros((rows2, 128), F32)
                brecv[slot, pl.ds(rows2, 1), :] = nothing
                brecv[slot, pl.ds(rows2 + 1, 1), :] = jnp.zeros((1, 128), F32)

    by_row(answer)

    own_query = two_maps(qbuf[y].astype(F32))
    own_key = kvbuf[y, pl.ds(0, 1), :].astype(BF16).astype(F32)
    own_value = kvbuf[y, pl.ds(1, 1), :].astype(BF16).astype(F32)
    own_score = to_row(jnp.sum(own_query * own_key, axis=1, keepdims=True) * scale)

    by_row(lambda reach: all_of(brecv.at[pl.ds(0, 2 * reach + 1)], 4).wait_recv())
    parts = [brecv[i] for i in range(5)]
    highs = [part[rows2 : rows2 + 1] for part in parts]
    high = functools.reduce(jnp.maximum, highs)
    count = jnp.zeros_like(high)
    weighted = jnp.zeros((rows2, 128), F32)
    for part, one in zip(parts, highs):
        factor = jnp.exp(one - high)
        count = count + factor * part[rows2 + 1 :]
        weighted = weighted + to_column(factor) * part[:rows2]
    zwsend[...] = weighted.astype(BF16)
    zstsend[...] = jnp.concatenate([high, count], axis=0)
    for target in range(nz):
        send(zstsend, zst.at[z], 6, {"kv_0": target, "tp": other})
        send(zwsend, zw.at[z], 5, {"kv_0": target, "tp": other})
    all_of(zst, 6).wait_recv()
    stats = [zst[k] for k in range(nz)]
    high = own_score
    for stat in stats:
        high = jnp.maximum(high, stat[:1])
    own_weight = jnp.exp(own_score - high)
    count = own_weight
    factors = []
    for stat in stats:
        factor = jnp.exp(stat[:1] - high)
        factors.append(factor)
        count = count + factor * stat[1:]
    share = 1.0 / count
    attention = to_column(own_weight * share) * own_value
    columns_of = [to_column(factor * share) for factor in factors]
    all_of(zw, 5).wait_recv()
    for k in range(nz):
        attention = attention + columns_of[k] * zw[k].astype(F32)
    gaps = attention[:heads] - lam * attention[heads:]
    mean = jnp.sum(gaps * gaps, axis=1, keepdims=True) / 128
    attended = gaps * lax.rsqrt(mean + epsilon) * hgain[...] * output_scale
    attbuf[core * ny + y] = attended.astype(BF16)
    mine = attbuf.at[core * ny + y]
    for k in far_first(ny):
        send(mine, mine, 7, {"kv_1": y_at(k)})
        send(mine, mine, 7, {"kv_1": y_at(k), "tp": other})
    send(mine, mine, 7, {"tp": other})

    all_of(kvbuf.at[pl.ds(0, ny - 1)], 3).wait_recv()
    for s in range(ny):
        out_ref[pl.ds(s, 1), pl.ds(128, 128)] = kvbuf[s, pl.ds(0, 1), :]
        out_ref[pl.ds(s, 1), pl.ds(256, 128)] = kvbuf[s, pl.ds(1, 1), :]
    all_of(outw.at[0], 8).wait_recv()

    all_of(attbuf.at[pl.ds(0, 2 * ny - 1)], 7).wait_recv()
    mixed = jnp.zeros((ny, 128), F32)
    for group in range(2):
        rows = jnp.concatenate(
            [attbuf[group * ny + s].astype(F32) for s in range(ny)], axis=0
        ).astype(BF16)
        product = lax.dot_general(
            rows, outw[group], (((1,), (1,)), ((), ())), preferred_element_type=F32
        )
        out_row = lax.broadcasted_iota(jnp.int32, product.shape, 0)
        out_lane = lax.broadcasted_iota(jnp.int32, product.shape, 1)
        product = jnp.where(lax.rem(out_row, heads) == out_lane // columns, product, 0.0)
        summed = jnp.sum(product.reshape(ny, heads, 128), axis=1)
        step = columns
        while step < 128:
            summed = summed + pltpu.roll(summed, step, 1)
            step *= 2
        mixed = mixed + summed.astype(BF16).astype(F32)
    out_ref[:, pl.ds(0, 128)] = mixed

    for which, ref in (
        (0, yrecv),
        (5, zw),
        (6, zst),
        (7, attbuf.at[pl.ds(0, 2 * ny - 1)]),
        (8, outw.at[0]),
    ):
        all_of(ref, which).wait_send()

    @pl.when(core == 0)
    def _():
        all_of(zbuf.at[pl.ds(0, nz)], 1).wait_send()

    @pl.when(core == 1)
    def _():
        all_of(zbuf.at[pl.ds(0, nz - 1)], 1).wait_send()
        all_of(qother, 15).wait_send()
        all_of(kvother, 13).wait_send()
        all_of(kvbuf.at[pl.ds(0, ny - 1)], 16).wait_send()
        all_of(kvbuf.at[pl.ds(0, ny - 1)], 3).wait_send()

    def drain(reach):
        @pl.when(core == 1)
        def _():
            all_of(qbuf.at[pl.ds(0, 2 * reach)], 2).wait_send()
            all_of(qbuf.at[pl.ds(0, 2 * reach)], 14).wait_send()

        all_of(brecv.at[pl.ds(0, 2 * reach + 1)], 4).wait_send()
        for side in range(2):
            all_of(kside.at[side, pl.ds(0, rows_at(reach))], 9 + side).wait_send()
            all_of(vside.at[side, pl.ds(0, rows_at(reach))], 11 + side).wait_send()

    by_row(drain)


def cut(x_ref, mixed_ref, nk_ref, nv_ref):
    mixed_ref[...] = x_ref[:, : mixed_ref.shape[1]].astype(BF16)
    nk_ref[...] = x_ref[:, 128:256].astype(BF16)
    nv_ref[...] = x_ref[:, 256:].astype(BF16)


def body(
    nz,
    ny,
    tokens,
    lengths,
    query_weight,
    key_weight,
    value_weight,
    query_gain,
    key_gain,
    lambdas,
    head_gain,
    out_weight,
    cache_keys,
    cache_values,
):
    sequences, positions = cache_keys.shape[:2]
    depth, width_q = query_weight.shape
    heads = width_q // 128
    rows2 = 2 * heads
    columns = out_weight.shape[1]
    half = query_gain.shape[0] // 2
    frequency = rotary_base ** (-np.arange(half, dtype=np.float64) / half)
    freq = jnp.asarray(np.tile(frequency, 4).astype(np.float32)[None, :])
    blocks = heads + 2
    any_space = pl.BlockSpec(memory_space=pl.ANY)
    vmem = pl.BlockSpec(memory_space=pltpu.VMEM)
    out = pl.pallas_call(
        functools.partial(kernel, nz, ny),
        name="decode_step",
        out_shape=pltpu.VMEM((sequences, 384), F32),
        in_specs=[any_space] * 13,
        out_specs=vmem,
        scratch_shapes=[
            pltpu.VMEM((sequences, depth), BF16),
            pltpu.VMEM((depth, width_q + 256), BF16),
            pltpu.SMEM((sequences,), jnp.int32),
            pltpu.VMEM((2, 1, 64), F32),
            pltpu.SMEM((heads,), F32),
            pltpu.VMEM((1, 128), F32),
            pltpu.VMEM((1, 128), F32),
            pltpu.VMEM((2, heads * columns, 128), BF16),
            pltpu.VMEM((sequences, positions, 128), BF16),
            pltpu.VMEM((sequences, positions, 128), BF16),
            pltpu.VMEM((sequences, blocks, 128), F32),
            pltpu.VMEM((ny, blocks, 128), F32),
            pltpu.VMEM((blocks, 128), F32),
            pltpu.VMEM((2 * nz, blocks, 128), F32),
            pltpu.VMEM((heads, 128), BF16),
            pltpu.VMEM((2, 128), F32),
            pltpu.VMEM((ny, heads, 128), BF16),
            pltpu.VMEM((ny, 2, 128), F32),
            pltpu.VMEM((2, 5 * positions // 2, 128), BF16),
            pltpu.VMEM((2, 5 * positions // 2, 128), BF16),
            pltpu.VMEM((ny, rows2 + 2, 128), F32),
            pltpu.VMEM((5, rows2 + 2, 128), F32),
            pltpu.VMEM((rows2, 128), BF16),
            pltpu.VMEM((2, 128), F32),
            pltpu.VMEM((nz, rows2, 128), BF16),
            pltpu.VMEM((nz, 2, 128), F32),
            pltpu.VMEM((2 * ny, heads, 128), BF16),
            pltpu.SemaphoreType.DMA((12 + heads,)),
            pltpu.SemaphoreType.DMA((17,)),
            pltpu.SemaphoreType.DMA((17,)),
            pltpu.SemaphoreType.DMA((ny,)),
            pltpu.SemaphoreType.REGULAR((2,)),
        ],
        compiler_params=pltpu.CompilerParams(collective_id=0, has_side_effects=True),
    )(
        tokens,
        lengths,
        query_weight,
        key_weight,
        value_weight,
        query_gain.reshape(1, -1),
        key_gain.reshape(1, -1),
        lambdas,
        head_gain.reshape(1, -1),
        out_weight.T,
        cache_keys.reshape(sequences, positions, 128),
        cache_values.reshape(sequences, positions, 128),
        freq,
    )
    mixed, new_keys, new_values = pl.pallas_call(
        cut,
        name="cut",
        out_shape=(
            jax.ShapeDtypeStruct((sequences, columns), BF16),
            jax.ShapeDtypeStruct((sequences, 128), BF16),
            jax.ShapeDtypeStruct((sequences, 128), BF16),
        ),
        in_specs=[vmem],
        out_specs=(vmem, vmem, vmem),
    )(pltpu.with_memory_space_constraint(out, pltpu.VMEM))
    return (
        mixed,
        new_keys.reshape(sequences, 1, 128),
        new_values.reshape(sequences, 1, 128),
    )


def solution(mesh):
    ny = 8
    nz = mesh.shape["kv"] // ny
    finer = Mesh(
        mesh.devices.reshape(mesh.shape["dp"], nz, ny, mesh.shape["tp"]),
        ("dp", "kv_0", "kv_1", "tp"),
    )
    in_specs = (
        P("dp", KV),
        P("dp"),
        P(KV, "tp"),
        P(KV, "tp"),
        P(KV, "tp"),
        P(),
        P(),
        P("tp"),
        P(),
        P("tp", KV),
        P("dp", KV, "tp", None),
        P("dp", KV, "tp", None),
    )
    out_specs = (P("dp", KV), P("dp", "tp", None), P("dp", "tp", None))
    return jax.shard_map(
        functools.partial(body, nz, ny),
        mesh=finer,
        in_specs=in_specs,
        out_specs=out_specs,
        check_vma=False,
    )
```

```python
import functools
import math

import jax
import jax.numpy as jnp
import numpy as np
from jax import lax
from jax.experimental import pallas as pl
from jax.experimental.pallas import tpu as pltpu
from jax.sharding import Mesh
from jax.sharding import PartitionSpec as P

KV = ("kv_0", "kv_1")
MESH = pl.DeviceIdType.MESH

epsilon = 1e-06
rotary_base = 10000.0
masked_score = -1e30
output_scale = 0.2 + 0.6 * math.exp(-0.3)
F32 = jnp.float32
BF16 = jnp.bfloat16


def far_first(n):
    return sorted(range(1, n), key=lambda k: -min(k, n - k))


def kernel(
    nz,
    ny,
    tok_hbm,
    len_hbm,
    wq_hbm,
    wk_hbm,
    wv_hbm,
    qg_hbm,
    kg_hbm,
    lam_hbm,
    hg_hbm,
    ow_hbm,
    ck_hbm,
    cv_hbm,
    freq_hbm,
    out_ref,
    tok,
    wts,
    lens,
    gains,
    lams,
    hgain,
    freq,
    outw,
    ck,
    cv,
    pbuf,
    yrecv,
    zsend,
    zbuf,
    qother,
    kvother,
    qbuf,
    kvbuf,
    kside,
    vside,
    bmsg,
    brecv,
    zwsend,
    zstsend,
    zw,
    zst,
    attbuf,
    load_sem,
    send_sem,
    recv_sem,
    q_sem,
    gate_sem,
):
    y = lax.axis_index("kv_1")
    z = lax.axis_index("kv_0")
    core = lax.axis_index("tp")
    other = 1 - core
    late = nz * 5 // 8
    positions = ck.shape[1]

    def y_at(k):
        return lax.rem(y + k, ny)

    def z_at(k):
        return lax.rem(z + k, nz)

    barrier = pltpu.get_barrier_semaphore()
    for k in far_first(ny):
        pl.semaphore_signal(barrier, 1, device_id={"kv_1": y_at(k), "tp": 1}, device_id_type=MESH)
    pl.semaphore_signal(barrier, 1, device_id={"tp": other}, device_id_type=MESH)
    for k in far_first(nz):
        pl.semaphore_signal(barrier, 1, device_id={"kv_0": z_at(k), "tp": 0}, device_id_type=MESH)

    width_q = wq_hbm.shape[1]
    loads = [
        pltpu.make_async_copy(tok_hbm, tok, load_sem.at[0]),
        pltpu.make_async_copy(wq_hbm, wts.at[:, pl.ds(0, width_q)], load_sem.at[1]),
        pltpu.make_async_copy(wk_hbm, wts.at[:, pl.ds(width_q, 128)], load_sem.at[2]),
        pltpu.make_async_copy(wv_hbm, wts.at[:, pl.ds(width_q + 128, 128)], load_sem.at[3]),
        pltpu.make_async_copy(len_hbm, lens, load_sem.at[4]),
        pltpu.make_async_copy(qg_hbm, gains.at[0], load_sem.at[5]),
        pltpu.make_async_copy(kg_hbm, gains.at[1], load_sem.at[6]),
        pltpu.make_async_copy(lam_hbm, lams, load_sem.at[7]),
        pltpu.make_async_copy(hg_hbm, hgain, load_sem.at[8]),
        pltpu.make_async_copy(freq_hbm, freq, load_sem.at[9]),
        pltpu.make_async_copy(ck_hbm, ck, load_sem.at[10]),
        pltpu.make_async_copy(cv_hbm, cv, load_sem.at[11]),
    ]
    heads = width_q // 128
    columns = ow_hbm.shape[0]
    for h in range(heads):
        loads.append(
            pltpu.make_async_copy(
                ow_hbm.at[:, pl.ds(128 * h, 128)],
                outw.at[core, pl.ds(columns * h, columns)],
                load_sem.at[12],
            )
        )
    for load in loads:
        load.start()

    def tell_other(gate):
        pl.semaphore_signal(gate_sem.at[gate], 1, device_id={"tp": other}, device_id_type=MESH)

    def send(src, dst, which, target, recv=None):
        copy = pltpu.make_async_remote_copy(
            src_ref=src,
            dst_ref=dst,
            send_sem=send_sem.at[which],
            recv_sem=recv_sem.at[which] if recv is None else recv,
            device_id=target,
            device_id_type=MESH,
        )
        copy.start()

    def all_of(ref, which):
        return pltpu.make_async_remote_copy(
            src_ref=ref,
            dst_ref=ref,
            send_sem=send_sem.at[which],
            recv_sem=recv_sem.at[which % 14],
            device_id={"tp": other},
            device_id_type=MESH,
        )

    for load in loads[:4]:
        load.wait()
    partial = jnp.dot(tok[...], wts[...], preferred_element_type=F32)
    blocks = heads + 2
    for c in range(blocks):
        pbuf[:, c, :] = partial[:, 128 * c : 128 * (c + 1)]

    @pl.when(core == 1)
    def _():
        pl.semaphore_wait(barrier, 2 * (ny - 1) + 1)
        tell_other(0)

    @pl.when(core == 0)
    def _():
        pl.semaphore_wait(gate_sem.at[0], 1)

    for k in far_first(ny):
        send(pbuf.at[y_at(k)], yrecv.at[k], 0, {"kv_1": y_at(k), "tp": other})
    send(pbuf.at[y], yrecv.at[0], 0, {"tp": other})
    half = positions // 2
    sides = ((0, 1), (1, ny - 1))
    middle = ny // 2

    def rows_at(reach):
        return (middle - reach - 1) * positions + half

    def move(reach):
        for d in range(middle, reach, -1):
            hops = d - reach
            for side, sign in sides:
                target = {"kv_1": y_at(hops * sign)}
                s = y_at(d * sign)
                rows_in = pl.ds(side * half, half) if d == middle else pl.ds(0, positions)
                rows_out = pl.ds((hops - 1) * positions, half if d == middle else positions)
                send(ck_hbm.at[s, rows_in], kside.at[side, rows_out], 9 + side, target)
                send(cv_hbm.at[s, rows_in], vside.at[side, rows_out], 11 + side, target)

    def by_row(step):
        @pl.when(z < late)
        def _():
            step(1)

        @pl.when(z >= late)
        def _():
            step(2)

    by_row(move)

    for load in loads[4:10]:
        load.wait()
    lane = lax.broadcasted_iota(jnp.int32, (blocks, 128), 1)
    row = lax.broadcasted_iota(jnp.int32, (blocks, 128), 0)
    gain_q = jnp.concatenate([gains[0], gains[0]], axis=1)
    gain_k = jnp.concatenate([gains[1], gains[1]], axis=1)
    gain = jnp.where(row < heads, gain_q, gain_k)
    angle = lens[y].astype(F32) * freq[...]
    cosine = jnp.cos(angle)
    sine = jnp.sin(angle)
    head_row = lax.broadcasted_iota(jnp.int32, (heads, 128), 0)
    lam = jnp.zeros((heads, 128), F32)
    for h in range(heads):
        lam = jnp.where(head_row == h, lams[h], lam)

    @pl.when(core == 0)
    def _():
        pl.semaphore_wait(barrier, 2 * (nz - 1) + 1)
        tell_other(1)

    @pl.when(core == 1)
    def _():
        pl.semaphore_wait(gate_sem.at[1], 1)

    pltpu.make_async_copy(outw.at[core], outw.at[core], load_sem.at[12]).wait()
    send(outw.at[core], outw.at[core], 8, {"tp": other})

    all_of(yrecv, 0).wait_recv()
    total = yrecv[0]
    for k in range(1, ny):
        total = total + yrecv[k]

    zsend[...] = total
    for k in far_first(nz):
        send(zsend, zbuf.at[other * nz + z], 1, {"kv_0": z_at(k), "tp": 1})

    @pl.when(core == 0)
    def _():
        send(zsend, zbuf.at[other * nz + z], 1, {"tp": 1})

    @pl.when(core == 1)
    def _():
        zbuf[z] = total
        all_of(zbuf.at[pl.ds(0, 2 * nz - 1)], 1).wait_recv()
        low = lane < 64
        for group in range(2):
            proj = zbuf[group * nz]
            for k in range(1, nz):
                proj = proj + zbuf[group * nz + k]
            squares = proj * proj
            mean_low = jnp.sum(jnp.where(low, squares, 0.0), axis=1, keepdims=True) / 64
            mean_high = jnp.sum(jnp.where(low, 0.0, squares), axis=1, keepdims=True) / 64
            inverse = jnp.where(
                low, lax.rsqrt(mean_low + epsilon), lax.rsqrt(mean_high + epsilon)
            )
            normed = proj * inverse * gain
            partner = jnp.where(
                lax.rem(lane, 64) < 32, -pltpu.roll(normed, 96, 1), pltpu.roll(normed, 32, 1)
            )
            rotated = normed * cosine + partner * sine
            query = rotated[:heads].astype(BF16)
            entry = jnp.concatenate(
                [rotated[heads : heads + 1], proj[heads + 1 :]], axis=0
            )
            if group == 0:
                qother[...] = query
                kvother[...] = entry
            else:
                qbuf[y] = query
                kvbuf[y] = entry

    def ask(reach):
        @pl.when(core == 1)
        def _():
            for e in range(reach, 0, -1):
                for _, sign in sides:
                    k = e * sign % ny
                    target = {"kv_1": y_at(k), "tp": 0}
                    send(qother, qbuf.at[y], 14, target, q_sem.at[k - 1])
            for e in range(reach, 0, -1):
                for _, sign in sides:
                    k = e * sign % ny
                    send(qbuf.at[y], qbuf.at[y], 2, {"kv_1": y_at(k)}, q_sem.at[k - 1])

    by_row(ask)

    @pl.when(core == 1)
    def _():
        send(qother, qbuf.at[y], 15, {"tp": 0}, q_sem.at[ny - 1])
        send(kvother, kvbuf.at[y], 13, {"tp": 0})
        for k in far_first(ny):
            target = {"kv_1": y_at(k), "tp": 0}
            send(kvother, kvbuf.at[y], 16, target, recv_sem.at[3])
            send(kvbuf.at[y], kvbuf.at[y], 3, {"kv_1": y_at(k)})

    scale = 64 ** (-0.5)
    rows2 = 2 * heads
    wide_lane = lax.broadcasted_iota(jnp.int32, (rows2, 128), 1)
    wide_row = lax.broadcasted_iota(jnp.int32, (rows2, 128), 0)
    eye = wide_lane == wide_row
    half_low = lax.broadcasted_iota(jnp.int32, (heads, 128), 1) < 64
    position = lax.broadcasted_iota(jnp.int32, (rows2, positions), 1)

    def positions_of(where):
        return position + (z * ny + where) * positions

    def positions_beside(side, reach):
        parts = [positions_of(y)]
        for hops in range(1, middle - reach + 1):
            parts.append(positions_of(y_at(hops if side == 1 else ny - hops)))
        parts[-1] = parts[-1][:, side * half : (side + 1) * half]
        return jnp.concatenate(parts, axis=1)

    def to_row(column):
        return jnp.sum(jnp.where(eye, column, 0.0), axis=0, keepdims=True)

    def to_column(values):
        return jnp.sum(jnp.where(eye, values, 0.0), axis=1, keepdims=True)

    def two_maps(query):
        return jnp.concatenate(
            [jnp.where(half_low, query, 0.0), jnp.where(half_low, 0.0, query)], axis=0
        )

    def attend(s, blocks, where):
        query = two_maps(qbuf[s].astype(F32)).astype(BF16)
        scores = [
            lax.dot_general(query, keys, (((1,), (1,)), ((), ())), preferred_element_type=F32)
            for keys, _ in blocks
        ]
        scores = jnp.concatenate(scores, axis=1) * scale
        valid = where < lens[s]
        highest = jnp.max(jnp.where(valid, scores, masked_score), axis=1, keepdims=True)
        expo = jnp.where(valid, jnp.exp(scores - highest), 0.0)
        count = jnp.sum(expo, axis=1, keepdims=True)
        expo = expo.astype(BF16)
        at = 0
        weighted = jnp.zeros((rows2, 128), F32)
        for _, values in blocks:
            part = expo[:, at : at + values.shape[0]]
            weighted = weighted + jnp.dot(part, values, preferred_element_type=F32)
            at += values.shape[0]
        bmsg[s, pl.ds(0, rows2), :] = weighted
        bmsg[s, pl.ds(rows2, 2), :] = jnp.concatenate([to_row(highest), to_row(count)], axis=0)

    for load in loads[10:12]:
        load.wait()
    @pl.when(core == 0)
    def _():
        pltpu.make_async_remote_copy(
            src_ref=qother,
            dst_ref=qbuf.at[y],
            send_sem=send_sem.at[15],
            recv_sem=q_sem.at[ny - 1],
            device_id={"tp": other},
            device_id_type=MESH,
        ).wait_recv()
        all_of(kvother, 13).wait_recv()

    attend(y, [(ck[y], cv[y])], positions_of(y))
    send(bmsg.at[y], brecv.at[4], 4, {"tp": other})

    def answer(reach):
        for e in range(1, reach + 1):
            for side, sign in sides:
                k = e * sign % ny
                s = y_at(k)
                pltpu.make_async_remote_copy(
                    src_ref=qbuf.at[s],
                    dst_ref=qbuf.at[s],
                    send_sem=send_sem.at[2],
                    recv_sem=q_sem.at[ny - k - 1],
                    device_id={"kv_1": s},
                    device_id_type=MESH,
                ).wait_recv()
                blocks, where = [(ck[s], cv[s])], positions_of(y)
                if e == reach:
                    keys = kside.at[side, pl.ds(0, rows_at(reach))]
                    values = vside.at[side, pl.ds(0, rows_at(reach))]
                    all_of(keys, 9 + side).wait_recv()
                    all_of(values, 11 + side).wait_recv()
                    blocks.append((keys[...], values[...]))
                    where = positions_beside(side, reach)
                attend(s, blocks, where)
                send(bmsg.at[s], brecv.at[2 * (e - 1) + side], 4, {"kv_1": s, "tp": other})
        if reach == 1:
            nothing = jnp.full((1, 128), masked_score, F32)
            for slot in (2, 3):
                brecv[slot, pl.ds(0, rows2), :] = jnp.zeros((rows2, 128), F32)
                brecv[slot, pl.ds(rows2, 1), :] = nothing
                brecv[slot, pl.ds(rows2 + 1, 1), :] = jnp.zeros((1, 128), F32)

    by_row(answer)

    own_query = two_maps(qbuf[y].astype(F32))
    own_key = kvbuf[y, pl.ds(0, 1), :].astype(BF16).astype(F32)
    own_value = kvbuf[y, pl.ds(1, 1), :].astype(BF16).astype(F32)
    own_score = to_row(jnp.sum(own_query * own_key, axis=1, keepdims=True) * scale)

    by_row(lambda reach: all_of(brecv.at[pl.ds(0, 2 * reach + 1)], 4).wait_recv())
    parts = [brecv[i] for i in range(5)]
    highs = [part[rows2 : rows2 + 1] for part in parts]
    high = functools.reduce(jnp.maximum, highs)
    count = jnp.zeros_like(high)
    weighted = jnp.zeros((rows2, 128), F32)
    for part, one in zip(parts, highs):
        factor = jnp.exp(one - high)
        count = count + factor * part[rows2 + 1 :]
        weighted = weighted + to_column(factor) * part[:rows2]
    zwsend[...] = weighted.astype(BF16)
    zstsend[...] = jnp.concatenate([high, count], axis=0)
    for target in range(nz):
        send(zstsend, zst.at[z], 6, {"kv_0": target, "tp": other})
        send(zwsend, zw.at[z], 5, {"kv_0": target, "tp": other})
    all_of(zst, 6).wait_recv()
    stats = [zst[k] for k in range(nz)]
    high = own_score
    for stat in stats:
        high = jnp.maximum(high, stat[:1])
    own_weight = jnp.exp(own_score - high)
    count = own_weight
    factors = []
    for stat in stats:
        factor = jnp.exp(stat[:1] - high)
        factors.append(factor)
        count = count + factor * stat[1:]
    share = 1.0 / count
    attention = to_column(own_weight * share) * own_value
    columns_of = [to_column(factor * share) for factor in factors]
    all_of(zw, 5).wait_recv()
    for k in range(nz):
        attention = attention + columns_of[k] * zw[k].astype(F32)
    gaps = attention[:heads] - lam * attention[heads:]
    mean = jnp.sum(gaps * gaps, axis=1, keepdims=True) / 128
    attended = gaps * lax.rsqrt(mean + epsilon) * hgain[...] * output_scale
    attbuf[core * ny + y] = attended.astype(BF16)
    mine = attbuf.at[core * ny + y]
    for k in far_first(ny):
        send(mine, mine, 7, {"kv_1": y_at(k)})
        send(mine, mine, 7, {"kv_1": y_at(k), "tp": other})
    send(mine, mine, 7, {"tp": other})

    all_of(kvbuf.at[pl.ds(0, ny - 1)], 3).wait_recv()
    for s in range(ny):
        out_ref[pl.ds(s, 1), pl.ds(128, 128)] = kvbuf[s, pl.ds(0, 1), :]
        out_ref[pl.ds(s, 1), pl.ds(256, 128)] = kvbuf[s, pl.ds(1, 1), :]
    all_of(outw.at[0], 8).wait_recv()

    for which, ref in (
        (0, yrecv),
        (5, zw),
        (6, zst),
        (8, outw.at[0]),
    ):
        all_of(ref, which).wait_send()

    @pl.when(core == 0)
    def _():
        all_of(zbuf.at[pl.ds(0, nz)], 1).wait_send()

    @pl.when(core == 1)
    def _():
        all_of(zbuf.at[pl.ds(0, nz - 1)], 1).wait_send()
        all_of(qother, 15).wait_send()
        all_of(kvother, 13).wait_send()
        all_of(kvbuf.at[pl.ds(0, ny - 1)], 16).wait_send()
        all_of(kvbuf.at[pl.ds(0, ny - 1)], 3).wait_send()

    def drain(reach):
        @pl.when(core == 1)
        def _():
            all_of(qbuf.at[pl.ds(0, 2 * reach)], 2).wait_send()
            all_of(qbuf.at[pl.ds(0, 2 * reach)], 14).wait_send()

        all_of(brecv.at[pl.ds(0, 2 * reach + 1)], 4).wait_send()
        for side in range(2):
            all_of(kside.at[side, pl.ds(0, rows_at(reach))], 9 + side).wait_send()
            all_of(vside.at[side, pl.ds(0, rows_at(reach))], 11 + side).wait_send()

    by_row(drain)

    all_of(attbuf.at[pl.ds(0, 2 * ny - 1)], 7).wait_recv()
    mixed = jnp.zeros((ny, 128), F32)
    for group in range(2):
        rows = jnp.concatenate(
            [attbuf[group * ny + s].astype(F32) for s in range(ny)], axis=0
        ).astype(BF16)
        product = lax.dot_general(
            rows, outw[group], (((1,), (1,)), ((), ())), preferred_element_type=F32
        )
        out_row = lax.broadcasted_iota(jnp.int32, product.shape, 0)
        out_lane = lax.broadcasted_iota(jnp.int32, product.shape, 1)
        product = jnp.where(lax.rem(out_row, heads) == out_lane // columns, product, 0.0)
        summed = jnp.sum(product.reshape(ny, heads, 128), axis=1)
        step = columns
        while step < 128:
            summed = summed + pltpu.roll(summed, step, 1)
            step *= 2
        mixed = mixed + summed.astype(BF16).astype(F32)
    out_ref[:, pl.ds(0, 128)] = mixed

    all_of(attbuf.at[pl.ds(0, 2 * ny - 1)], 7).wait_send()


def cut(x_ref, mixed_ref, nk_ref, nv_ref):
    mixed_ref[...] = x_ref[:, : mixed_ref.shape[1]].astype(BF16)
    nk_ref[...] = x_ref[:, 128:256].astype(BF16)
    nv_ref[...] = x_ref[:, 256:].astype(BF16)


def body(
    nz,
    ny,
    tokens,
    lengths,
    query_weight,
    key_weight,
    value_weight,
    query_gain,
    key_gain,
    lambdas,
    head_gain,
    out_weight,
    cache_keys,
    cache_values,
):
    sequences, positions = cache_keys.shape[:2]
    depth, width_q = query_weight.shape
    heads = width_q // 128
    rows2 = 2 * heads
    columns = out_weight.shape[1]
    half = query_gain.shape[0] // 2
    frequency = rotary_base ** (-np.arange(half, dtype=np.float64) / half)
    freq = jnp.asarray(np.tile(frequency, 4).astype(np.float32)[None, :])
    blocks = heads + 2
    any_space = pl.BlockSpec(memory_space=pl.ANY)
    vmem = pl.BlockSpec(memory_space=pltpu.VMEM)
    out = pl.pallas_call(
        functools.partial(kernel, nz, ny),
        name="decode_step",
        out_shape=pltpu.VMEM((sequences, 384), F32),
        in_specs=[any_space] * 13,
        out_specs=vmem,
        scratch_shapes=[
            pltpu.VMEM((sequences, depth), BF16),
            pltpu.VMEM((depth, width_q + 256), BF16),
            pltpu.SMEM((sequences,), jnp.int32),
            pltpu.VMEM((2, 1, 64), F32),
            pltpu.SMEM((heads,), F32),
            pltpu.VMEM((1, 128), F32),
            pltpu.VMEM((1, 128), F32),
            pltpu.VMEM((2, heads * columns, 128), BF16),
            pltpu.VMEM((sequences, positions, 128), BF16),
            pltpu.VMEM((sequences, positions, 128), BF16),
            pltpu.VMEM((sequences, blocks, 128), F32),
            pltpu.VMEM((ny, blocks, 128), F32),
            pltpu.VMEM((blocks, 128), F32),
            pltpu.VMEM((2 * nz, blocks, 128), F32),
            pltpu.VMEM((heads, 128), BF16),
            pltpu.VMEM((2, 128), F32),
            pltpu.VMEM((ny, heads, 128), BF16),
            pltpu.VMEM((ny, 2, 128), F32),
            pltpu.VMEM((2, 5 * positions // 2, 128), BF16),
            pltpu.VMEM((2, 5 * positions // 2, 128), BF16),
            pltpu.VMEM((ny, rows2 + 2, 128), F32),
            pltpu.VMEM((5, rows2 + 2, 128), F32),
            pltpu.VMEM((rows2, 128), BF16),
            pltpu.VMEM((2, 128), F32),
            pltpu.VMEM((nz, rows2, 128), BF16),
            pltpu.VMEM((nz, 2, 128), F32),
            pltpu.VMEM((2 * ny, heads, 128), BF16),
            pltpu.SemaphoreType.DMA((13,)),
            pltpu.SemaphoreType.DMA((17,)),
            pltpu.SemaphoreType.DMA((14,)),
            pltpu.SemaphoreType.DMA((ny,)),
            pltpu.SemaphoreType.REGULAR((2,)),
        ],
        compiler_params=pltpu.CompilerParams(collective_id=0, has_side_effects=True),
    )(
        tokens,
        lengths,
        query_weight,
        key_weight,
        value_weight,
        query_gain.reshape(1, -1),
        key_gain.reshape(1, -1),
        lambdas,
        head_gain.reshape(1, -1),
        out_weight.T,
        cache_keys.reshape(sequences, positions, 128),
        cache_values.reshape(sequences, positions, 128),
        freq,
    )
    mixed, new_keys, new_values = pl.pallas_call(
        cut,
        name="cut",
        out_shape=(
            jax.ShapeDtypeStruct((sequences, columns), BF16),
            jax.ShapeDtypeStruct((sequences, 128), BF16),
            jax.ShapeDtypeStruct((sequences, 128), BF16),
        ),
        in_specs=[vmem],
        out_specs=(vmem, vmem, vmem),
    )(pltpu.with_memory_space_constraint(out, pltpu.VMEM))
    return (
        mixed,
        new_keys.reshape(sequences, 1, 128),
        new_values.reshape(sequences, 1, 128),
    )


def solution(mesh):
    ny = 8
    nz = mesh.shape["kv"] // ny
    finer = Mesh(
        mesh.devices.reshape(mesh.shape["dp"], nz, ny, mesh.shape["tp"]),
        ("dp", "kv_0", "kv_1", "tp"),
    )
    in_specs = (
        P("dp", KV),
        P("dp"),
        P(KV, "tp"),
        P(KV, "tp"),
        P(KV, "tp"),
        P(),
        P(),
        P("tp"),
        P(),
        P("tp", KV),
        P("dp", KV, "tp", None),
        P("dp", KV, "tp", None),
    )
    out_specs = (P("dp", KV), P("dp", "tp", None), P("dp", "tp", None))
    return jax.shard_map(
        functools.partial(body, nz, ny),
        mesh=finer,
        in_specs=in_specs,
        out_specs=out_specs,
        check_vma=False,
    )
```

```python
import functools
import math

import jax
import jax.numpy as jnp
import numpy as np
from jax import lax
from jax.experimental import pallas as pl
from jax.experimental.pallas import tpu as pltpu
from jax.sharding import Mesh
from jax.sharding import PartitionSpec as P

KV = ("kv_0", "kv_1")
MESH = pl.DeviceIdType.MESH

epsilon = 1e-06
rotary_base = 10000.0
masked_score = -1e30
output_scale = 0.2 + 0.6 * math.exp(-0.3)
F32 = jnp.float32
BF16 = jnp.bfloat16


def far_first(n):
    return sorted(range(1, n), key=lambda k: -min(k, n - k))


def kernel(
    nz,
    ny,
    tok_hbm,
    len_hbm,
    wq_hbm,
    wk_hbm,
    wv_hbm,
    qg_hbm,
    kg_hbm,
    lam_hbm,
    hg_hbm,
    ow_hbm,
    ck_hbm,
    cv_hbm,
    freq_hbm,
    out_ref,
    tok,
    wts,
    lens,
    gains,
    lams,
    hgain,
    freq,
    outw,
    ck,
    cv,
    pbuf,
    yrecv,
    zsend,
    zbuf,
    qother,
    kvother,
    qbuf,
    kvbuf,
    kside,
    vside,
    bmsg,
    brecv,
    zwsend,
    zstsend,
    zw,
    zst,
    attbuf,
    load_sem,
    send_sem,
    recv_sem,
    q_sem,
    gate_sem,
):
    y = lax.axis_index("kv_1")
    z = lax.axis_index("kv_0")
    core = lax.axis_index("tp")
    other = 1 - core
    late = nz * 5 // 8
    positions = ck.shape[1]

    def y_at(k):
        return lax.rem(y + k, ny)

    def z_at(k):
        return lax.rem(z + k, nz)

    barrier = pltpu.get_barrier_semaphore()
    for k in far_first(ny):
        pl.semaphore_signal(barrier, 1, device_id={"kv_1": y_at(k), "tp": 1}, device_id_type=MESH)
    pl.semaphore_signal(barrier, 1, device_id={"tp": other}, device_id_type=MESH)

    width_q = wq_hbm.shape[1]
    loads = [
        pltpu.make_async_copy(tok_hbm, tok, load_sem.at[0]),
        pltpu.make_async_copy(wq_hbm, wts.at[:, pl.ds(0, width_q)], load_sem.at[1]),
        pltpu.make_async_copy(wk_hbm, wts.at[:, pl.ds(width_q, 128)], load_sem.at[2]),
        pltpu.make_async_copy(wv_hbm, wts.at[:, pl.ds(width_q + 128, 128)], load_sem.at[3]),
        pltpu.make_async_copy(len_hbm, lens, load_sem.at[4]),
        pltpu.make_async_copy(qg_hbm, gains.at[0], load_sem.at[5]),
        pltpu.make_async_copy(kg_hbm, gains.at[1], load_sem.at[6]),
        pltpu.make_async_copy(lam_hbm, lams, load_sem.at[7]),
        pltpu.make_async_copy(hg_hbm, hgain, load_sem.at[8]),
        pltpu.make_async_copy(freq_hbm, freq, load_sem.at[9]),
        pltpu.make_async_copy(ck_hbm, ck, load_sem.at[10]),
        pltpu.make_async_copy(cv_hbm, cv, load_sem.at[11]),
    ]
    heads = width_q // 128
    columns = ow_hbm.shape[0]
    for h in range(heads):
        loads.append(
            pltpu.make_async_copy(
                ow_hbm.at[:, pl.ds(128 * h, 128)],
                outw.at[core, pl.ds(columns * h, columns)],
                load_sem.at[12],
            )
        )
    for load in loads[:4]:
        load.start()
    for k in far_first(nz):
        pl.semaphore_signal(barrier, 1, device_id={"kv_0": z_at(k), "tp": 0}, device_id_type=MESH)
    for load in loads[4:]:
        load.start()

    def tell_other(gate):
        pl.semaphore_signal(gate_sem.at[gate], 1, device_id={"tp": other}, device_id_type=MESH)

    def send(src, dst, which, target, recv=None):
        copy = pltpu.make_async_remote_copy(
            src_ref=src,
            dst_ref=dst,
            send_sem=send_sem.at[which],
            recv_sem=recv_sem.at[which] if recv is None else recv,
            device_id=target,
            device_id_type=MESH,
        )
        copy.start()

    def all_of(ref, which):
        return pltpu.make_async_remote_copy(
            src_ref=ref,
            dst_ref=ref,
            send_sem=send_sem.at[which],
            recv_sem=recv_sem.at[which % 14],
            device_id={"tp": other},
            device_id_type=MESH,
        )

    for load in loads[:4]:
        load.wait()
    partial = jnp.dot(tok[...], wts[...], preferred_element_type=F32)
    blocks = heads + 2
    for c in range(blocks):
        pbuf[:, c, :] = partial[:, 128 * c : 128 * (c + 1)]

    @pl.when(core == 1)
    def _():
        pl.semaphore_wait(barrier, 2 * (ny - 1) + 1)
        tell_other(0)

    @pl.when(core == 0)
    def _():
        pl.semaphore_wait(gate_sem.at[0], 1)

    for k in far_first(ny):
        send(pbuf.at[y_at(k)], yrecv.at[k], 0, {"kv_1": y_at(k), "tp": other})
    send(pbuf.at[y], yrecv.at[0], 0, {"tp": other})
    half = positions // 2
    sides = ((0, 1), (1, ny - 1))
    middle = ny // 2

    def rows_at(reach):
        return (middle - reach - 1) * positions + half

    def move(reach):
        for d in range(middle, reach, -1):
            hops = d - reach
            for side, sign in sides:
                target = {"kv_1": y_at(hops * sign)}
                s = y_at(d * sign)
                rows_in = pl.ds(side * half, half) if d == middle else pl.ds(0, positions)
                rows_out = pl.ds((hops - 1) * positions, half if d == middle else positions)
                send(ck_hbm.at[s, rows_in], kside.at[side, rows_out], 9 + side, target)
                send(cv_hbm.at[s, rows_in], vside.at[side, rows_out], 11 + side, target)

    def by_row(step):
        @pl.when(z < late)
        def _():
            step(1)

        @pl.when(z >= late)
        def _():
            step(2)

    by_row(move)

    for load in loads[4:10]:
        load.wait()
    lane = lax.broadcasted_iota(jnp.int32, (blocks, 128), 1)
    row = lax.broadcasted_iota(jnp.int32, (blocks, 128), 0)
    gain_q = jnp.concatenate([gains[0], gains[0]], axis=1)
    gain_k = jnp.concatenate([gains[1], gains[1]], axis=1)
    gain = jnp.where(row < heads, gain_q, gain_k)
    angle = lens[y].astype(F32) * freq[...]
    cosine = jnp.cos(angle)
    sine = jnp.sin(angle)
    head_row = lax.broadcasted_iota(jnp.int32, (heads, 128), 0)
    lam = jnp.zeros((heads, 128), F32)
    for h in range(heads):
        lam = jnp.where(head_row == h, lams[h], lam)

    @pl.when(core == 0)
    def _():
        pl.semaphore_wait(barrier, 2 * (nz - 1) + 1)
        tell_other(1)

    @pl.when(core == 1)
    def _():
        pl.semaphore_wait(gate_sem.at[1], 1)

    pltpu.make_async_copy(outw.at[core], outw.at[core], load_sem.at[12]).wait()
    send(outw.at[core], outw.at[core], 8, {"tp": other})

    all_of(yrecv, 0).wait_recv()
    total = yrecv[0]
    for k in range(1, ny):
        total = total + yrecv[k]

    zsend[...] = total
    for k in far_first(nz):
        send(zsend, zbuf.at[other * nz + z], 1, {"kv_0": z_at(k), "tp": 1})

    @pl.when(core == 0)
    def _():
        send(zsend, zbuf.at[other * nz + z], 1, {"tp": 1})

    @pl.when(core == 1)
    def _():
        zbuf[z] = total
        all_of(zbuf.at[pl.ds(0, 2 * nz - 1)], 1).wait_recv()
        low = lane < 64
        for group in range(2):
            proj = zbuf[group * nz]
            for k in range(1, nz):
                proj = proj + zbuf[group * nz + k]
            squares = proj * proj
            mean_low = jnp.sum(jnp.where(low, squares, 0.0), axis=1, keepdims=True) / 64
            mean_high = jnp.sum(jnp.where(low, 0.0, squares), axis=1, keepdims=True) / 64
            inverse = jnp.where(
                low, lax.rsqrt(mean_low + epsilon), lax.rsqrt(mean_high + epsilon)
            )
            normed = proj * inverse * gain
            partner = jnp.where(
                lax.rem(lane, 64) < 32, -pltpu.roll(normed, 96, 1), pltpu.roll(normed, 32, 1)
            )
            rotated = normed * cosine + partner * sine
            query = rotated[:heads].astype(BF16)
            entry = jnp.concatenate(
                [rotated[heads : heads + 1], proj[heads + 1 :]], axis=0
            )
            if group == 0:
                qother[...] = query
                kvother[...] = entry
            else:
                qbuf[y] = query
                kvbuf[y] = entry

    def ask(reach):
        @pl.when(core == 1)
        def _():
            for e in range(reach, 0, -1):
                for _, sign in sides:
                    k = e * sign % ny
                    target = {"kv_1": y_at(k), "tp": 0}
                    send(qother, qbuf.at[y], 14, target, q_sem.at[k - 1])
            for e in range(reach, 0, -1):
                for _, sign in sides:
                    k = e * sign % ny
                    send(qbuf.at[y], qbuf.at[y], 2, {"kv_1": y_at(k)}, q_sem.at[k - 1])

    by_row(ask)

    @pl.when(core == 1)
    def _():
        send(qother, qbuf.at[y], 15, {"tp": 0}, q_sem.at[ny - 1])
        send(kvother, kvbuf.at[y], 13, {"tp": 0})
        for k in far_first(ny):
            target = {"kv_1": y_at(k), "tp": 0}
            send(kvother, kvbuf.at[y], 16, target, recv_sem.at[3])
            send(kvbuf.at[y], kvbuf.at[y], 3, {"kv_1": y_at(k)})

    scale = 64 ** (-0.5)
    rows2 = 2 * heads
    wide_lane = lax.broadcasted_iota(jnp.int32, (rows2, 128), 1)
    wide_row = lax.broadcasted_iota(jnp.int32, (rows2, 128), 0)
    eye = wide_lane == wide_row
    half_low = lax.broadcasted_iota(jnp.int32, (heads, 128), 1) < 64
    position = lax.broadcasted_iota(jnp.int32, (rows2, positions), 1)

    def positions_of(where):
        return position + (z * ny + where) * positions

    def positions_beside(side, reach):
        parts = [positions_of(y)]
        for hops in range(1, middle - reach + 1):
            parts.append(positions_of(y_at(hops if side == 1 else ny - hops)))
        parts[-1] = parts[-1][:, side * half : (side + 1) * half]
        return jnp.concatenate(parts, axis=1)

    def to_row(column):
        return jnp.sum(jnp.where(eye, column, 0.0), axis=0, keepdims=True)

    def to_column(values):
        return jnp.sum(jnp.where(eye, values, 0.0), axis=1, keepdims=True)

    def two_maps(query):
        return jnp.concatenate(
            [jnp.where(half_low, query, 0.0), jnp.where(half_low, 0.0, query)], axis=0
        )

    def attend(s, blocks, where):
        query = two_maps(qbuf[s].astype(F32)).astype(BF16)
        scores = [
            lax.dot_general(query, keys, (((1,), (1,)), ((), ())), preferred_element_type=F32)
            for keys, _ in blocks
        ]
        scores = jnp.concatenate(scores, axis=1) * scale
        valid = where < lens[s]
        highest = jnp.max(jnp.where(valid, scores, masked_score), axis=1, keepdims=True)
        expo = jnp.where(valid, jnp.exp(scores - highest), 0.0)
        count = jnp.sum(expo, axis=1, keepdims=True)
        expo = expo.astype(BF16)
        at = 0
        weighted = jnp.zeros((rows2, 128), F32)
        for _, values in blocks:
            part = expo[:, at : at + values.shape[0]]
            weighted = weighted + jnp.dot(part, values, preferred_element_type=F32)
            at += values.shape[0]
        bmsg[s, pl.ds(0, rows2), :] = weighted
        bmsg[s, pl.ds(rows2, 2), :] = jnp.concatenate([to_row(highest), to_row(count)], axis=0)

    for load in loads[10:12]:
        load.wait()
    @pl.when(core == 0)
    def _():
        pltpu.make_async_remote_copy(
            src_ref=qother,
            dst_ref=qbuf.at[y],
            send_sem=send_sem.at[15],
            recv_sem=q_sem.at[ny - 1],
            device_id={"tp": other},
            device_id_type=MESH,
        ).wait_recv()
        all_of(kvother, 13).wait_recv()

    attend(y, [(ck[y], cv[y])], positions_of(y))
    send(bmsg.at[y], brecv.at[4], 4, {"tp": other})

    def answer(reach):
        for e in range(1, reach + 1):
            for side, sign in sides:
                k = e * sign % ny
                s = y_at(k)
                pltpu.make_async_remote_copy(
                    src_ref=qbuf.at[s],
                    dst_ref=qbuf.at[s],
                    send_sem=send_sem.at[2],
                    recv_sem=q_sem.at[ny - k - 1],
                    device_id={"kv_1": s},
                    device_id_type=MESH,
                ).wait_recv()
                blocks, where = [(ck[s], cv[s])], positions_of(y)
                if e == reach:
                    keys = kside.at[side, pl.ds(0, rows_at(reach))]
                    values = vside.at[side, pl.ds(0, rows_at(reach))]
                    all_of(keys, 9 + side).wait_recv()
                    all_of(values, 11 + side).wait_recv()
                    blocks.append((keys[...], values[...]))
                    where = positions_beside(side, reach)
                attend(s, blocks, where)
                send(bmsg.at[s], brecv.at[2 * (e - 1) + side], 4, {"kv_1": s, "tp": other})
        if reach == 1:
            nothing = jnp.full((1, 128), masked_score, F32)
            for slot in (2, 3):
                brecv[slot, pl.ds(0, rows2), :] = jnp.zeros((rows2, 128), F32)
                brecv[slot, pl.ds(rows2, 1), :] = nothing
                brecv[slot, pl.ds(rows2 + 1, 1), :] = jnp.zeros((1, 128), F32)

    by_row(answer)

    own_query = two_maps(qbuf[y].astype(F32))
    own_key = kvbuf[y, pl.ds(0, 1), :].astype(BF16).astype(F32)
    own_value = kvbuf[y, pl.ds(1, 1), :].astype(BF16).astype(F32)
    own_score = to_row(jnp.sum(own_query * own_key, axis=1, keepdims=True) * scale)

    by_row(lambda reach: all_of(brecv.at[pl.ds(0, 2 * reach + 1)], 4).wait_recv())
    parts = [brecv[i] for i in range(5)]
    highs = [part[rows2 : rows2 + 1] for part in parts]
    high = functools.reduce(jnp.maximum, highs)
    count = jnp.zeros_like(high)
    weighted = jnp.zeros((rows2, 128), F32)
    for part, one in zip(parts, highs):
        factor = jnp.exp(one - high)
        count = count + factor * part[rows2 + 1 :]
        weighted = weighted + to_column(factor) * part[:rows2]
    zwsend[...] = weighted.astype(BF16)
    zstsend[...] = jnp.concatenate([high, count], axis=0)
    for target in range(nz):
        send(zstsend, zst.at[z], 6, {"kv_0": target, "tp": other})
        send(zwsend, zw.at[z], 5, {"kv_0": target, "tp": other})
    all_of(zst, 6).wait_recv()
    all_of(zw, 5).wait_recv()
    stats = [zst[k] for k in range(nz)]
    high = own_score
    for stat in stats:
        high = jnp.maximum(high, stat[:1])
    own_weight = jnp.exp(own_score - high)
    count = own_weight
    factors = []
    for stat in stats:
        factor = jnp.exp(stat[:1] - high)
        factors.append(factor)
        count = count + factor * stat[1:]
    share = 1.0 / count
    attention = to_column(own_weight * share) * own_value
    columns_of = [to_column(factor * share) for factor in factors]
    for k in range(nz):
        attention = attention + columns_of[k] * zw[k].astype(F32)
    gaps = attention[:heads] - lam * attention[heads:]
    mean = jnp.sum(gaps * gaps, axis=1, keepdims=True) / 128
    attended = gaps * lax.rsqrt(mean + epsilon) * hgain[...] * output_scale
    attbuf[core * ny + y] = attended.astype(BF16)
    mine = attbuf.at[core * ny + y]
    for k in far_first(ny):
        send(mine, mine, 7, {"kv_1": y_at(k), "tp": 1})
    send(mine, mine, 7, {"tp": other})
    for k in far_first(ny):
        send(mine, mine, 7, {"kv_1": y_at(k), "tp": 0})

    all_of(kvbuf.at[pl.ds(0, ny - 1)], 3).wait_recv()
    for s in range(ny):
        out_ref[pl.ds(s, 1), pl.ds(128, 128)] = kvbuf[s, pl.ds(0, 1), :]
        out_ref[pl.ds(s, 1), pl.ds(256, 128)] = kvbuf[s, pl.ds(1, 1), :]
    all_of(outw.at[0], 8).wait_recv()

    for which, ref in (
        (0, yrecv),
        (5, zw),
        (6, zst),
        (8, outw.at[0]),
    ):
        all_of(ref, which).wait_send()

    @pl.when(core == 0)
    def _():
        all_of(zbuf.at[pl.ds(0, nz)], 1).wait_send()

    @pl.when(core == 1)
    def _():
        all_of(zbuf.at[pl.ds(0, nz - 1)], 1).wait_send()
        all_of(qother, 15).wait_send()
        all_of(kvother, 13).wait_send()
        all_of(kvbuf.at[pl.ds(0, ny - 1)], 16).wait_send()
        all_of(kvbuf.at[pl.ds(0, ny - 1)], 3).wait_send()

    def drain(reach):
        @pl.when(core == 1)
        def _():
            all_of(qbuf.at[pl.ds(0, 2 * reach)], 2).wait_send()
            all_of(qbuf.at[pl.ds(0, 2 * reach)], 14).wait_send()

        all_of(brecv.at[pl.ds(0, 2 * reach + 1)], 4).wait_send()
        for side in range(2):
            all_of(kside.at[side, pl.ds(0, rows_at(reach))], 9 + side).wait_send()
            all_of(vside.at[side, pl.ds(0, rows_at(reach))], 11 + side).wait_send()

    by_row(drain)

    all_of(attbuf.at[pl.ds(0, 2 * ny - 1)], 7).wait_recv()
    mixed = jnp.zeros((ny, 128), F32)
    for group in range(2):
        rows = jnp.concatenate(
            [attbuf[group * ny + s].astype(F32) for s in range(ny)], axis=0
        ).astype(BF16)
        product = lax.dot_general(
            rows, outw[group], (((1,), (1,)), ((), ())), preferred_element_type=F32
        )
        out_row = lax.broadcasted_iota(jnp.int32, product.shape, 0)
        out_lane = lax.broadcasted_iota(jnp.int32, product.shape, 1)
        product = jnp.where(lax.rem(out_row, heads) == out_lane // columns, product, 0.0)
        summed = jnp.sum(product.reshape(ny, heads, 128), axis=1)
        step = columns
        while step < 128:
            summed = summed + pltpu.roll(summed, step, 1)
            step *= 2
        mixed = mixed + summed.astype(BF16).astype(F32)
    out_ref[:, pl.ds(0, 128)] = mixed

    all_of(attbuf.at[pl.ds(0, 2 * ny - 1)], 7).wait_send()


def cut(x_ref, mixed_ref, nk_ref, nv_ref):
    mixed_ref[...] = x_ref[:, : mixed_ref.shape[1]].astype(BF16)
    nk_ref[...] = x_ref[:, 128:256].astype(BF16)
    nv_ref[...] = x_ref[:, 256:].astype(BF16)


def body(
    nz,
    ny,
    tokens,
    lengths,
    query_weight,
    key_weight,
    value_weight,
    query_gain,
    key_gain,
    lambdas,
    head_gain,
    out_weight,
    cache_keys,
    cache_values,
):
    sequences, positions = cache_keys.shape[:2]
    depth, width_q = query_weight.shape
    heads = width_q // 128
    rows2 = 2 * heads
    columns = out_weight.shape[1]
    half = query_gain.shape[0] // 2
    frequency = rotary_base ** (-np.arange(half, dtype=np.float64) / half)
    freq = jnp.asarray(np.tile(frequency, 4).astype(np.float32)[None, :])
    blocks = heads + 2
    any_space = pl.BlockSpec(memory_space=pl.ANY)
    vmem = pl.BlockSpec(memory_space=pltpu.VMEM)
    out = pl.pallas_call(
        functools.partial(kernel, nz, ny),
        name="decode_step",
        out_shape=pltpu.VMEM((sequences, 384), F32),
        in_specs=[any_space] * 13,
        out_specs=vmem,
        scratch_shapes=[
            pltpu.VMEM((sequences, depth), BF16),
            pltpu.VMEM((depth, width_q + 256), BF16),
            pltpu.SMEM((sequences,), jnp.int32),
            pltpu.VMEM((2, 1, 64), F32),
            pltpu.SMEM((heads,), F32),
            pltpu.VMEM((1, 128), F32),
            pltpu.VMEM((1, 128), F32),
            pltpu.VMEM((2, heads * columns, 128), BF16),
            pltpu.VMEM((sequences, positions, 128), BF16),
            pltpu.VMEM((sequences, positions, 128), BF16),
            pltpu.VMEM((sequences, blocks, 128), F32),
            pltpu.VMEM((ny, blocks, 128), F32),
            pltpu.VMEM((blocks, 128), F32),
            pltpu.VMEM((2 * nz, blocks, 128), F32),
            pltpu.VMEM((heads, 128), BF16),
            pltpu.VMEM((2, 128), F32),
            pltpu.VMEM((ny, heads, 128), BF16),
            pltpu.VMEM((ny, 2, 128), F32),
            pltpu.VMEM((2, 5 * positions // 2, 128), BF16),
            pltpu.VMEM((2, 5 * positions // 2, 128), BF16),
            pltpu.VMEM((ny, rows2 + 2, 128), F32),
            pltpu.VMEM((5, rows2 + 2, 128), F32),
            pltpu.VMEM((rows2, 128), BF16),
            pltpu.VMEM((2, 128), F32),
            pltpu.VMEM((nz, rows2, 128), BF16),
            pltpu.VMEM((nz, 2, 128), F32),
            pltpu.VMEM((2 * ny, heads, 128), BF16),
            pltpu.SemaphoreType.DMA((13,)),
            pltpu.SemaphoreType.DMA((17,)),
            pltpu.SemaphoreType.DMA((14,)),
            pltpu.SemaphoreType.DMA((ny,)),
            pltpu.SemaphoreType.REGULAR((2,)),
        ],
        compiler_params=pltpu.CompilerParams(collective_id=0, has_side_effects=True),
    )(
        tokens,
        lengths,
        query_weight,
        key_weight,
        value_weight,
        query_gain.reshape(1, -1),
        key_gain.reshape(1, -1),
        lambdas,
        head_gain.reshape(1, -1),
        out_weight.T,
        cache_keys.reshape(sequences, positions, 128),
        cache_values.reshape(sequences, positions, 128),
        freq,
    )
    mixed, new_keys, new_values = pl.pallas_call(
        cut,
        name="cut",
        out_shape=(
            jax.ShapeDtypeStruct((sequences, columns), BF16),
            jax.ShapeDtypeStruct((sequences, 128), BF16),
            jax.ShapeDtypeStruct((sequences, 128), BF16),
        ),
        in_specs=[vmem],
        out_specs=(vmem, vmem, vmem),
    )(pltpu.with_memory_space_constraint(out, pltpu.VMEM))
    return (
        mixed,
        new_keys.reshape(sequences, 1, 128),
        new_values.reshape(sequences, 1, 128),
    )


def solution(mesh):
    ny = 8
    nz = mesh.shape["kv"] // ny
    finer = Mesh(
        mesh.devices.reshape(mesh.shape["dp"], nz, ny, mesh.shape["tp"]),
        ("dp", "kv_0", "kv_1", "tp"),
    )
    in_specs = (
        P("dp", KV),
        P("dp"),
        P(KV, "tp"),
        P(KV, "tp"),
        P(KV, "tp"),
        P(),
        P(),
        P("tp"),
        P(),
        P("tp", KV),
        P("dp", KV, "tp", None),
        P("dp", KV, "tp", None),
    )
    out_specs = (P("dp", KV), P("dp", "tp", None), P("dp", "tp", None))
    return jax.shard_map(
        functools.partial(body, nz, ny),
        mesh=finer,
        in_specs=in_specs,
        out_specs=out_specs,
        check_vma=False,
    )
```
